32 devices in a mesh: ep: 8 (over z, x), tp: 4 (over y, core).
Axes of the slice: x: 2, y: 2, z: 4, core: 2. Of those that a mesh axis runs over, the one named last changes fastest.
Arguments:
- tokens: bfloat16 [4096, 2048], P(('ep', 'tp')), may hold values from -6 to 6
- routes: int32 [4096, 2], P(('ep', 'tp')), may hold values from 0 to 31, as said below
- gates: float32 [4096, 2], P(('ep', 'tp')), may hold values from 0.1 to 0.6
- w_gate: bfloat16 [32, 2048, 768], P(('ep', 'tp')), may hold values from -0.125 to 0.125
- w_up: bfloat16 [32, 2048, 768], P(('ep', 'tp')), may hold values from -0.125 to 0.125
- w_down: bfloat16 [32, 768, 2048], P(('ep', 'tp')), may hold values from -0.21875 to 0.21875
- moe_out: bfloat16 [4096, 2048], P('ep', 'tp'), may hold values from -16 to 16
- norm_gain: float32 [2048], P('tp'), may hold values from 0.1 to 1.9
- out_grad: bfloat16 [4096, 2048], P('ep', 'tp'), may hold values from -16 to 16
Outputs:
- token_grad: bfloat16 [4096, 2048], P(('ep', 'tp'))
- gates_grad: bfloat16 [4096, 2], P(('ep', 'tp'))
- w_gate_grad: bfloat16 [32, 2048, 768], P(('ep', 'tp'))
- w_up_grad: bfloat16 [32, 2048, 768], P(('ep', 'tp'))
- w_down_grad: bfloat16 [32, 768, 2048], P(('ep', 'tp'))
The draws below stay inside these ranges and needn't reach their ends.
Inputs may be any that keep to these rules, and one draw needn't show every extreme that they name: `routes`: the two experts of a row differ and lie in one group (expert e is in group e // 8). In the 128 rows of one device the tokens fall into the groups in shares 3/8, 3/8, 1/8, 1/8 of 128, which group takes which share varying. In the rows of one device no expert is named more than 16 times, and one expert is named exactly 16 times in the rows of every device.
All inputs are finite; a program needn't handle non-finite values.
Results may differ from the reference program's by a relative error of at most 0.0071.
Values may be sent and summed in bfloat16 or wider, within the bound.
No kernel may reach another device: no remote copies, remote signals or barrier semaphores. Data moves between devices by JAX's collectives and lax.ppermute only.
A program may use at most 128 MiB of HBM per device.

```python
import jax
import jax.numpy as jnp
from jax import lax

D = 2048
F = 768
GROUPS = 4
TOPK = 2
TOK_DEV = 128
EXPERTS = 32
EXP_GROUP = 8
CAP = 16
TOKENS = 4096


def draw_routes(key, part):
    tickets = EXP_GROUP * CAP
    shares = [3 * TOK_DEV // 8, 3 * TOK_DEV // 8, TOK_DEV // 8, TOK_DEV // 8]
    hot_global = jax.random.randint(jax.random.fold_in(key, 11), (), 0, EXPERTS)

    def one_block(block_key):
        sub_keys = jax.random.split(block_key, 4)
        group_order = jax.random.permutation(sub_keys[0], GROUPS)
        token_order = jax.random.permutation(sub_keys[1], TOK_DEV)
        hot_inner = jax.random.randint(sub_keys[2], (GROUPS,), 0, EXP_GROUP)
        noise_draw = jax.random.randint(sub_keys[3], (GROUPS, tickets), 0, 2 ** 19)
        ticket_ids = jnp.arange(tickets, dtype=jnp.int32)
        inner_ids = ticket_ids // CAP
        result = jnp.zeros((TOK_DEV, 2), jnp.int32)
        offset = 0
        for rank in range(GROUPS):
            expert_ids = group_order[rank] * EXP_GROUP + inner_ids
            hot_flag = jnp.logical_or(inner_ids == hot_inner[rank], expert_ids == hot_global).astype(jnp.int32)
            score_value = (hot_flag * 2 ** 19 + noise_draw[rank]) * tickets + ticket_ids
            share_size = shares[rank]
            picked = lax.top_k(score_value, 2 * share_size)[1]
            chosen = jnp.sort(expert_ids[picked])
            places = token_order[offset:offset + share_size]
            result = result.at[places, 0].set(chosen[:share_size])
            result = result.at[places, 1].set(chosen[share_size:])
            offset = offset + share_size
        return result
    block_keys = jax.random.split(jax.random.fold_in(key, 12), TOKENS // TOK_DEV)
    return jax.vmap(one_block)(block_keys).reshape(TOKENS, 2).astype(jnp.int32)


def paired_fields(key):
    sub_keys = jax.random.split(jax.random.fold_in(key, 21), 5)
    base = jax.random.normal(sub_keys[0], (TOKENS, D), jnp.float32)
    block_scale = jnp.exp(jax.random.uniform(sub_keys[1], (8,), jnp.float32, -1.2, 1.2))
    fine_scale = jnp.exp(jax.random.uniform(sub_keys[2], (D,), jnp.float32, -0.35, 0.35))
    columns = jnp.arange(D) * 8 // D
    col_scale = block_scale[columns] * fine_scale
    saved_out = jnp.clip(base * col_scale[None, :], -16.0, 16.0)
    noise_part = jax.random.normal(sub_keys[4], (TOKENS, D), jnp.float32)
    cotangent = jnp.clip(0.6 * base + 0.8 * noise_part, -16.0, 16.0)
    return (saved_out, cotangent)


def draw_moe_out(key, part):
    return paired_fields(key)[0].astype(jnp.bfloat16)


def draw_out_grad(key, part):
    return paired_fields(key)[1].astype(jnp.bfloat16)


def steps_of(key, shape, pieces, smallest, high):
    def one(dim, parts):
        draws = jax.random.uniform(jax.random.fold_in(jax.random.fold_in(key, 6), dim), (parts,), jnp.float32, smallest / len(pieces), high / len(pieces))
        return jnp.repeat(jnp.exp(draws), shape[dim] // parts).reshape((-1,) + (1,) * (len(shape) - dim - 1))

    loudness = one(*pieces[0])
    for cut in pieces[1:]:
        loudness = loudness * one(*cut)
    return loudness


def gaussian(key, extent, deviation, limit, shards=(), held_as=jnp.bfloat16):
    values = deviation * jax.random.normal(key, extent, jnp.float32)
    if shards:
        values = values * steps_of(key, extent, shards, -0.22, 0.18)
    return jnp.clip(values, -limit, limit).astype(held_as)


def setup_inputs(seed: int = 0) -> dict:
    arg_keys = jax.random.split(jax.random.key(seed), 10)
    tokens = gaussian(arg_keys[0], (TOKENS, D), 1.0, 6.0, ((0, 32),))
    routes = draw_routes(jax.random.fold_in(arg_keys[9], 71), 0)
    gates = jnp.clip(0.1 + 0.5 * jax.random.uniform(arg_keys[2], (TOKENS, TOPK), jnp.float32) ** steps_of(arg_keys[2], (TOKENS, TOPK), ((0, 32),), -0.2, 0.2), 0.1, 0.6)
    w_gate = gaussian(arg_keys[3], (EXPERTS, D, F), D ** -0.5, 0.125, ((0, 32),))
    w_up = gaussian(arg_keys[4], (EXPERTS, D, F), D ** -0.5, 0.125, ((0, 32),))
    w_down = gaussian(arg_keys[5], (EXPERTS, F, D), F ** -0.5, 0.21875, ((0, 32),))
    moe_out = draw_moe_out(jax.random.fold_in(arg_keys[9], 71), 0)
    norm_gain = jnp.clip(1.0 + 0.18 * jax.random.normal(arg_keys[7], (D,), jnp.float32), 0.1, 1.9)
    out_grad = draw_out_grad(jax.random.fold_in(arg_keys[9], 71), 0)
    return {"tokens": tokens, "routes": routes, "gates": gates, "w_gate": w_gate, "w_up": w_up, "w_down": w_down, "moe_out": moe_out, "norm_gain": norm_gain, "out_grad": out_grad}


epsilon = 1e-06
block_rows = 256

def contract(left, right, left_dim, right_dim):
    return lax.dot_general(left, right, (((left_dim,), (right_dim,)), ((), ())), preferred_element_type=jnp.float32)

def norm_backward(moe_out, norm_gain, out_grad):
    features = moe_out.shape[1]
    saved_out = moe_out.astype(jnp.float32)
    scaled = norm_gain.astype(jnp.float32)[None, :] * out_grad.astype(jnp.float32)
    square_sum = lax.optimization_barrier(jnp.sum(saved_out * saved_out, axis=1))
    cross_sum = lax.optimization_barrier(jnp.sum(saved_out * scaled, axis=1))
    inv_rms = lax.rsqrt(square_sum / features + epsilon)
    result = inv_rms[:, None] * scaled - saved_out * (inv_rms ** 3 * cross_sum / features)[:, None]
    return result.astype(jnp.bfloat16)

def expert_terms(row_block, cot_block, gate_row, w_gate_one, w_up_one, w_down_one):
    pre_gate = jnp.dot(row_block, w_gate_one, preferred_element_type=jnp.float32)
    pre_up = jnp.dot(row_block, w_up_one, preferred_element_type=jnp.float32)
    sigmoid_gate = jax.nn.sigmoid(pre_gate)
    activated = pre_gate * sigmoid_gate
    hidden = activated * pre_up
    hid_grad = contract(cot_block, w_down_one, 1, 1)
    gate_grad = lax.optimization_barrier(jnp.sum(hidden * hid_grad, axis=1)).astype(jnp.bfloat16)
    weight = gate_row.astype(jnp.float32)[:, None]
    d_hidden = weight * hid_grad
    d_gate = (d_hidden * pre_up * sigmoid_gate * (1.0 + pre_gate * (1.0 - sigmoid_gate))).astype(jnp.bfloat16)
    d_up = (d_hidden * activated).astype(jnp.bfloat16)
    token_back = (contract(d_gate, w_gate_one, 1, 1) + contract(d_up, w_up_one, 1, 1)).astype(jnp.bfloat16)
    scaled_cot = (weight * cot_block.astype(jnp.float32)).astype(jnp.bfloat16)
    grad_gate = contract(row_block, d_gate, 0, 0)
    grad_up = contract(row_block, d_up, 0, 0)
    grad_down = contract(hidden.astype(jnp.bfloat16), scaled_cot, 0, 0)
    return (token_back, gate_grad, grad_gate, grad_up, grad_down)

def reference(tokens, routes, gates, w_gate, w_up, w_down, moe_out, norm_gain, out_grad):
    features = tokens.shape[1]
    hidden_width = w_gate.shape[2]
    expert_cot = norm_backward(moe_out, norm_gain, out_grad)
    flat_ids = routes.reshape(-1).astype(jnp.int32)
    route_count = flat_ids.shape[0]
    flat_token = (jnp.arange(route_count, dtype=jnp.int32) // TOPK).astype(jnp.int32)
    flat_gate = gates.reshape(-1).astype(jnp.bfloat16)
    sorted_order = jnp.argsort(flat_ids, stable=True).astype(jnp.int32)
    totals = jnp.zeros((EXPERTS,), jnp.int32).at[flat_ids].add(1)
    starts = (jnp.cumsum(totals) - totals).astype(jnp.int32)
    token_pad = jnp.concatenate([tokens, jnp.zeros((1, features), jnp.bfloat16)], axis=0)
    cot_pad = jnp.concatenate([expert_cot, jnp.zeros((1, features), jnp.bfloat16)], axis=0)

    def per_expert(state_pair, inputs):
        expert_index, w_gate_one, w_up_one, w_down_one = inputs
        first_slot = starts[expert_index]
        load_size = totals[expert_index]

        def one_block(block_index, state):
            route_dx, route_gg, acc_gate, acc_up, acc_down = state
            position = (first_slot + block_index * block_rows + jnp.arange(block_rows, dtype=jnp.int32)).astype(jnp.int32)
            in_range = position < first_slot + load_size
            route_ids = sorted_order[jnp.clip(position, 0, route_count - 1)]
            token_ids = jnp.where(in_range, flat_token[route_ids], TOKENS).astype(jnp.int32)
            gate_row = jnp.where(in_range, flat_gate[route_ids], jnp.zeros((), jnp.bfloat16))
            target = jnp.where(in_range, route_ids, route_count).astype(jnp.int32)
            token_back, gate_grad, grad_gate, grad_up, grad_down = expert_terms(token_pad[token_ids], cot_pad[token_ids], gate_row, w_gate_one, w_up_one, w_down_one)
            route_dx = route_dx.at[target].set(token_back)
            route_gg = route_gg.at[target].set(gate_grad)
            return (route_dx, route_gg, acc_gate + grad_gate, acc_up + grad_up, acc_down + grad_down)
        blocks = (load_size + block_rows - 1) // block_rows
        start_state = (state_pair[0], state_pair[1], jnp.zeros((features, hidden_width), jnp.float32), jnp.zeros((features, hidden_width), jnp.float32), jnp.zeros((hidden_width, features), jnp.float32))
        route_dx, route_gg, acc_gate, acc_up, acc_down = lax.fori_loop(0, blocks, one_block, start_state)
        return ((route_dx, route_gg), (acc_gate.astype(jnp.bfloat16), acc_up.astype(jnp.bfloat16), acc_down.astype(jnp.bfloat16)))
    start_pair = (jnp.zeros((route_count + 1, features), jnp.bfloat16), jnp.zeros((route_count + 1,), jnp.bfloat16))
    final_pair, stacked = lax.scan(per_expert, start_pair, (jnp.arange(EXPERTS, dtype=jnp.int32), w_gate, w_up, w_down))
    route_dx, route_gg = final_pair
    token_grad = lax.optimization_barrier(jnp.sum(route_dx[:route_count].astype(jnp.float32).reshape(TOKENS, TOPK, features), axis=1)).astype(jnp.bfloat16)
    gates_grad = route_gg[:route_count].reshape(TOKENS, TOPK)
    return (token_grad, gates_grad, stacked[0], stacked[1], stacked[2])
```

```python
import functools

import jax
import jax.numpy as jnp
from jax import lax
from jax.experimental import pallas as pl
from jax.experimental.pallas import tpu as pltpu
from jax.sharding import PartitionSpec as P


epsilon = 1e-06
AXES = ("ep", "tp")
GROUPS = 4
META = 128
SETS = ((0, 1), (3, 2))
BF = jnp.bfloat16
F32 = jnp.float32


def contract(left, right, left_dim, right_dim):
    return lax.dot_general(
        left, right, (((left_dim,), (right_dim,)), ((), ())), preferred_element_type=F32
    )


def one_hot(column, width):
    lanes = lax.broadcasted_iota(jnp.int32, (column.shape[0], width), 1)
    return jnp.where(column == lanes, 1.0, 0.0).astype(BF)


def strict_lower(rows):
    above = lax.broadcasted_iota(jnp.int32, (rows, rows), 1)
    below = lax.broadcasted_iota(jnp.int32, (rows, rows), 0)
    return jnp.where(above < below, 1.0, 0.0).astype(BF)


def lane_of(column_values, rows):
    lanes = lax.broadcasted_iota(jnp.int32, (rows, META), 1)
    result = jnp.zeros((rows, META), F32)
    for lane, column in enumerate(column_values):
        result = jnp.where(lanes == lane, column, result)
    return result


def place(group_size):
    flat = lax.axis_index("ep") * lax.axis_size("tp") + lax.axis_index("tp")
    return lax.div(flat, group_size), lax.rem(flat, group_size)


def split_kernel(pieces, moe_ref, gain_ref, grad_ref, *out_refs):
    me = lax.axis_index("tp")
    width = moe_ref.shape[1]
    rows = moe_ref.shape[0] // pieces
    for index in range(pieces):
        first = pl.multiple_of(jnp.bitwise_xor(me, index) * rows, rows)
        grad = grad_ref[pl.ds(first, rows), :].astype(F32)
        out_refs[index][:, :width] = (gain_ref[...] * grad).astype(BF)
        out_refs[index][:, width:] = moe_ref[pl.ds(first, rows), :]


def token_pack_kernel(group_size, share, tok_ref, routes_ref, gates_ref, *out_refs):
    out_refs, hot_ref = out_refs[:-1], out_refs[-1]
    rows, features = tok_ref.shape
    plane, _ = place(group_size)
    first = routes_ref[:, 0:1]
    second = routes_ref[:, 1:2]
    group = lax.div(first, group_size)
    shift = lax.rem(group - plane + GROUPS, GROUPS)
    member = one_hot(shift, META)
    before = contract(strict_lower(rows), member, 1, 0)
    rank = jnp.sum(before * member.astype(F32), axis=1, keepdims=True).astype(jnp.int32)
    hot = one_hot(shift * share + rank, GROUPS * share)
    hot_ref[...] = hot
    base = group * group_size
    meta = lane_of(
        (
            (first - base + 1).astype(F32),
            (second - base + 1).astype(F32),
            gates_ref[:, 0:1],
            gates_ref[:, 1:2],
        ),
        rows,
    ).astype(BF)
    packed = contract(hot, tok_ref[...], 0, 0).astype(BF)
    packed_meta = contract(hot, meta, 0, 0).astype(BF)
    for index in range(GROUPS):
        out_refs[index][:, :features] = packed[index * share : (index + 1) * share]
        out_refs[index][:, features:] = packed_meta[index * share : (index + 1) * share]


def cot_pack_kernel(pieces, share, *refs):
    piece_refs, hot_ref = refs[:pieces], refs[pieces]
    out_refs, full_ref = refs[pieces + 1 : -1], refs[-1]
    me = lax.axis_index("tp")
    width = piece_refs[0].shape[1] // 2
    features = width * pieces
    square_sum = 0.0
    cross_sum = 0.0
    for ref in piece_refs:
        saved = ref[:, width:].astype(F32)
        scaled = ref[:, :width].astype(F32)
        square_sum += jnp.sum(saved * saved, axis=1, keepdims=True)
        cross_sum += jnp.sum(saved * scaled, axis=1, keepdims=True)
    inv_rms = lax.rsqrt(square_sum / features + epsilon)
    factor = inv_rms * inv_rms * inv_rms * cross_sum / features
    for index, ref in enumerate(piece_refs):
        saved = ref[:, width:].astype(F32)
        scaled = ref[:, :width].astype(F32)
        column = pl.multiple_of(jnp.bitwise_xor(me, index) * width, width)
        full_ref[:, pl.ds(column, width)] = (inv_rms * scaled - saved * factor).astype(BF)
    packed = contract(hot_ref[...], full_ref[...], 0, 0).astype(BF)
    for index in range(GROUPS):
        out_refs[index][...] = packed[index * share : (index + 1) * share]


def token_route_kernel(group_size, capacity, *refs):
    shifts = (len(refs) - group_size - 3) // 1
    msg_refs, out_refs = refs[:shifts], refs[shifts : shifts + group_size]
    hot0_ref, hot1_ref, full_ref = refs[-3:]
    share, width = msg_refs[0].shape
    features = width - META
    slots = shifts * capacity
    _, mine = place(group_size)
    lower = strict_lower(share)
    gates = []
    for index, ref in enumerate(msg_refs):
        row = slice(index * share, (index + 1) * share)
        full_ref[row, :] = ref[:, :features]
        meta = ref[:, features:].astype(F32)
        gates.append((meta[:, 2:3], meta[:, 3:4]))
        experts = [meta[:, k : k + 1].astype(jnp.int32) - 1 for k in range(2)]
        members = [one_hot(e, META) for e in experts]
        before = contract(lower, members[0] + members[1], 1, 0)
        for expert, member, hot_ref in zip(experts, members, (hot0_ref, hot1_ref)):
            rank = jnp.sum(before * member.astype(F32), axis=1, keepdims=True)
            slot = jnp.bitwise_xor(expert, mine) * slots + index * capacity
            slot = jnp.where(expert < 0, -1, slot + rank.astype(jnp.int32))
            hot_ref[row, :] = one_hot(slot, group_size * slots)
    hot0, hot1 = hot0_ref[...], hot1_ref[...]
    total = shifts * share
    gate0 = lane_of((jnp.concatenate([g[0] for g in gates], axis=0),), total).astype(BF)
    gate1 = lane_of((jnp.concatenate([g[1] for g in gates], axis=0),), total).astype(BF)
    packed_gate = contract(hot0, gate0, 0, 0) + contract(hot1, gate1, 0, 0)
    packed = contract(hot0 + hot1, full_ref[...], 0, 0)
    for index in range(group_size):
        row = slice(index * slots, (index + 1) * slots)
        out_refs[index][:, :features] = packed[row].astype(BF)
        out_refs[index][:, features:] = packed_gate[row].astype(BF)


def cot_route_kernel(group_size, *refs):
    shifts = len(refs) - group_size - 3
    msg_refs, hot0_ref, hot1_ref = refs[:shifts], refs[shifts], refs[shifts + 1]
    out_refs, full_ref = refs[shifts + 2 : -1], refs[-1]
    share = msg_refs[0].shape[0]
    slots = hot0_ref.shape[1] // group_size
    for index, ref in enumerate(msg_refs):
        full_ref[index * share : (index + 1) * share, :] = ref[...]
    packed = contract(hot0_ref[...] + hot1_ref[...], full_ref[...], 0, 0)
    for index in range(group_size):
        out_refs[index][...] = packed[index * slots : (index + 1) * slots].astype(BF)


def combine_kernel(group_size, shifts, *refs):
    piece_refs, hot0_ref, hot1_ref = refs[:group_size], refs[group_size], refs[group_size + 1]
    out_refs = refs[group_size + 2 :]
    features = piece_refs[0].shape[1] - META
    share = hot0_ref.shape[0] // shifts
    rows = jnp.concatenate([ref[...].astype(F32) for ref in piece_refs], axis=0).astype(BF)
    hot0, hot1 = hot0_ref[...], hot1_ref[...]
    summed = contract(hot0 + hot1, rows[:, :features], 1, 0).astype(BF)
    grad0 = contract(hot0, rows[:, features:], 1, 0)[:, 0:1]
    grad1 = contract(hot1, rows[:, features:], 1, 0)[:, 0:1]
    meta = lane_of((grad0, grad1), shifts * share).astype(BF)
    for index in range(shifts):
        row = slice(index * share, (index + 1) * share)
        out_refs[index][:, :features] = summed[row]
        out_refs[index][:, features:] = meta[row]


def finish_kernel(hot_ref, *refs):
    msg_refs, tok_ref, gates_ref = refs[:GROUPS], refs[-2], refs[-1]
    features = tok_ref.shape[1]
    rows = jnp.concatenate([ref[...] for ref in msg_refs], axis=0)
    hot = hot_ref[...]
    tok_ref[...] = contract(hot, rows[:, :features], 1, 0).astype(BF)
    gates_ref[...] = contract(hot, rows[:, features:], 1, 0)[:, 0:2].astype(BF)


def call(kernel, outs, args, scratch=(), flops=0):
    outs = [jax.ShapeDtypeStruct(shape, BF) for shape in outs]
    size = sum(a.size * a.dtype.itemsize for a in args) + sum(o.size * 2 for o in outs)
    return pl.pallas_call(
        kernel,
        out_shape=outs,
        in_specs=[pl.BlockSpec(memory_space=pltpu.VMEM)] * len(args),
        out_specs=[pl.BlockSpec(memory_space=pltpu.VMEM)] * len(outs),
        scratch_shapes=[pltpu.VMEM(shape, BF) for shape in scratch],
        cost_estimate=pl.CostEstimate(flops=flops, bytes_accessed=size, transcendentals=0),
    )(*args)


def local(tokens, routes, gates, w_gate, w_up, w_down, moe_out, norm_gain, out_grad):
    devices = lax.axis_size(AXES)
    pieces = lax.axis_size("tp")
    group_size = devices // GROUPS
    tok_rows, features = tokens.shape
    capacity = 4 * tok_rows // devices
    share = 3 * tok_rows // 8
    wide = features + META

    def over_tp(array, bits):
        pairs = [(d, d ^ bits) for d in range(pieces)]
        return lax.ppermute(array, "tp", pairs)

    def over_plane(array, bits):
        pairs = [
            (d, d // group_size * group_size + (d % group_size ^ bits)) for d in range(devices)
        ]
        return lax.ppermute(array, AXES, pairs)

    def over_z(array, shift):
        pairs = [(d, (d + shift * group_size) % devices) for d in range(devices)]
        return lax.ppermute(array, AXES, pairs)

    part = [(tok_rows, 2 * moe_out.shape[1])] * pieces
    split = call(
        functools.partial(split_kernel, pieces), part, (moe_out, norm_gain[None, :], out_grad)
    )
    *tok_msgs, hot = call(
        functools.partial(token_pack_kernel, group_size, share),
        [(share, wide)] * GROUPS + [(tok_rows, GROUPS * share)],
        (tokens, routes, gates),
        flops=2 * tok_rows * GROUPS * share * wide,
    )
    split = [split[0]] + [over_tp(split[m], m) for m in range(1, pieces)]
    order = [s for group in SETS for s in group]
    tok_at = {s: over_z(tok_msgs[s], s) if s else tok_msgs[s] for s in order}
    cot_msgs = call(
        functools.partial(cot_pack_kernel, pieces, share),
        [(share, features)] * GROUPS,
        (*split, hot),
        scratch=[(tok_rows, features)],
        flops=2 * tok_rows * GROUPS * share * features,
    )
    cot_at = {s: over_z(cot_msgs[s], s) if s else cot_msgs[s] for s in order}

    hots, tok_in, cot_in = [], [], []
    for group in SETS:
        count = len(group)
        slots = count * capacity
        *out, hot0, hot1 = call(
            functools.partial(token_route_kernel, group_size, capacity),
            [(slots, wide)] * group_size + [(count * share, group_size * slots)] * 2,
            [tok_at[s] for s in group],
            scratch=[(count * share, features)],
            flops=2 * count * share * group_size * slots * wide,
        )
        hots.append((hot0, hot1))
        tok_in.append([out[0]] + [over_plane(out[m], m) for m in range(1, group_size)])
    for group, (hot0, hot1) in zip(SETS, hots):
        count = len(group)
        slots = count * capacity
        out = call(
            functools.partial(cot_route_kernel, group_size),
            [(slots, features)] * group_size,
            [cot_at[s] for s in group] + [hot0, hot1],
            scratch=[(count * share, features)],
            flops=2 * count * share * group_size * slots * features,
        )
        cot_in.append([out[0]] + [over_plane(out[m], m) for m in range(1, group_size)])

    w_gate_one, w_up_one, w_down_one = w_gate[0], w_up[0], w_down[0]
    backs, kept = [], []
    for index, group in enumerate(SETS):
        slots = len(group) * capacity
        wide_rows = jnp.concatenate(tok_in[index], axis=0)
        row_block = wide_rows[:, :features]
        weight = wide_rows[:, features : features + 1].astype(F32)
        cot_rows = jnp.concatenate(cot_in[index], axis=0)
        pre_gate = jnp.dot(row_block, w_gate_one, preferred_element_type=F32)
        pre_up = jnp.dot(row_block, w_up_one, preferred_element_type=F32)
        sigmoid_gate = jax.nn.sigmoid(pre_gate)
        activated = pre_gate * sigmoid_gate
        hidden = activated * pre_up
        hid_grad = contract(cot_rows, w_down_one, 1, 1)
        gate_grad = jnp.sum(hidden * hid_grad, axis=1, keepdims=True).astype(BF)
        d_hidden = weight * hid_grad
        d_gate = (
            d_hidden * pre_up * sigmoid_gate * (1.0 + pre_gate * (1.0 - sigmoid_gate))
        ).astype(BF)
        d_up = (d_hidden * activated).astype(BF)
        token_back = (contract(d_gate, w_gate_one, 1, 1) + contract(d_up, w_up_one, 1, 1)).astype(
            BF
        )
        meta = jnp.pad(gate_grad, ((0, 0), (0, META - 1)))
        back = jnp.concatenate([token_back, meta], axis=1)
        back = [back[m * slots : (m + 1) * slots] for m in range(group_size)]
        backs.append([back[0]] + [over_plane(back[m], m) for m in range(1, group_size)])
        scaled_cot = (weight * cot_rows.astype(F32)).astype(BF)
        kept.append((row_block, d_gate, d_up, hidden.astype(BF), scaled_cot))

    rows, d_gate, d_up, hidden, scaled_cot = (jnp.concatenate(k, axis=0) for k in zip(*kept))
    grad_gate = contract(rows, d_gate, 0, 0).astype(BF)
    grad_up = contract(rows, d_up, 0, 0).astype(BF)
    grad_down = contract(hidden, scaled_cot, 0, 0).astype(BF)

    home = {}
    for group, back, (hot0, hot1) in zip(SETS, backs, hots):
        count = len(group)
        out = call(
            functools.partial(combine_kernel, group_size, count),
            [(share, wide)] * count,
            [*back, hot0, hot1],
            flops=2 * hot0.size * wide,
        )
        for s, array in zip(group, out):
            home[s] = over_z(array, -s) if s else array
    token_grad, gates_grad = call(
        finish_kernel,
        [(tok_rows, features), (tok_rows, routes.shape[1])],
        [hot] + [home[s] for s in range(GROUPS)],
        flops=2 * hot.size * wide,
    )
    return (token_grad, gates_grad, grad_gate[None], grad_up[None], grad_down[None])


def solution(mesh):
    in_specs = (
        P(AXES, None),
        P(AXES, None),
        P(AXES, None),
        P(AXES, None, None),
        P(AXES, None, None),
        P(AXES, None, None),
        P("ep", "tp"),
        P("tp"),
        P("ep", "tp"),
    )
    out_specs = (
        P(AXES, None),
        P(AXES, None),
        P(AXES, None, None),
        P(AXES, None, None),
        P(AXES, None, None),
    )
    return jax.shard_map(local, mesh=mesh, in_specs=in_specs, out_specs=out_specs, check_vma=False)
```

```python
import functools

import jax
import jax.numpy as jnp
from jax import lax
from jax.experimental import pallas as pl
from jax.experimental.pallas import tpu as pltpu
from jax.sharding import PartitionSpec as P


epsilon = 1e-06
AXES = ("ep", "tp")
GROUPS = 4
META = 128
GAIN_ROWS = 16
HIDDEN_TILES = 3
FEATURE_TILES = 4
SMALL_VMEM = 16 * 2**20
BIG_VMEM = 40 * 2**20
SETS = ((1, 2), (3, 0))
BF = jnp.bfloat16
F32 = jnp.float32


def contract(left, right, left_dim, right_dim):
    return lax.dot_general(
        left, right, (((left_dim,), (right_dim,)), ((), ())), preferred_element_type=F32
    )


def one_hot(column, width):
    lanes = lax.broadcasted_iota(jnp.int32, (column.shape[0], width), 1)
    return jnp.where(column == lanes, 1.0, 0.0).astype(BF)


def strict_lower(rows):
    above = lax.broadcasted_iota(jnp.int32, (rows, rows), 1)
    below = lax.broadcasted_iota(jnp.int32, (rows, rows), 0)
    return jnp.where(above < below, 1.0, 0.0).astype(BF)


def lane_of(column_values, rows):
    lanes = lax.broadcasted_iota(jnp.int32, (rows, META), 1)
    result = jnp.zeros((rows, META), F32)
    for lane, column in enumerate(column_values):
        result = jnp.where(lanes == lane, column, result)
    return result


def place(group_size):
    flat = lax.axis_index("ep") * lax.axis_size("tp") + lax.axis_index("tp")
    return lax.div(flat, group_size), lax.rem(flat, group_size)


def split_kernel(pieces, moe_ref, gain_ref, grad_ref, *out_refs):
    me = lax.axis_index("tp")
    width = moe_ref.shape[1]
    rows = moe_ref.shape[0] // pieces
    gain = gain_ref[...]
    high = gain.astype(BF).astype(F32)
    middle = (gain - high).astype(BF).astype(F32)
    low = gain - high - middle
    line = lax.broadcasted_iota(jnp.int32, (GAIN_ROWS, width), 0)
    parts = jnp.where(line == 0, high, jnp.where(line == 1, middle, 0.0))
    parts = jnp.where(line == 2, low, parts).astype(BF)
    for index in range(pieces):
        first = pl.multiple_of(jnp.bitwise_xor(me, index) * rows, rows)
        out_refs[index][:rows, :width] = grad_ref[pl.ds(first, rows), :]
        out_refs[index][:rows, width:] = moe_ref[pl.ds(first, rows), :]
        out_refs[index][rows:, :width] = parts
        out_refs[index][rows:, width:] = jnp.zeros((GAIN_ROWS, width), BF)


def token_pack_kernel(group_size, share, tok_ref, routes_ref, gates_ref, *refs):
    out_refs, hot_ref, rows_ref = refs[:-2], refs[-2], refs[-1]
    rows, features = tok_ref.shape
    plane, _ = place(group_size)
    rows_ref[...] = jnp.zeros_like(rows_ref)
    rows_ref[0:2, :] = routes_ref[...].astype(F32)
    rows_ref[2:4, :] = gates_ref[...]
    unit_row = lax.broadcasted_iota(jnp.int32, (rows, rows), 0)
    unit_col = lax.broadcasted_iota(jnp.int32, (rows, rows), 1)
    unit = jnp.where(unit_row == unit_col, 1.0, 0.0).astype(BF)
    columns = contract(unit, rows_ref[...].astype(BF), 1, 1)
    first = columns[:, 0:1].astype(jnp.int32)
    second = columns[:, 1:2].astype(jnp.int32)
    group = lax.div(first, group_size)
    shift = lax.rem(group - plane + GROUPS, GROUPS)
    member = one_hot(shift, META)
    before = contract(strict_lower(rows), member, 1, 0)
    rank = jnp.sum(before * member.astype(F32), axis=1, keepdims=True).astype(jnp.int32)
    hot = one_hot(shift * share + rank, GROUPS * share)
    hot_ref[...] = hot
    base = group * group_size
    meta = lane_of(
        (
            (first - base + 1).astype(F32),
            (second - base + 1).astype(F32),
            columns[:, 2:3],
            columns[:, 3:4],
        ),
        rows,
    ).astype(BF)
    packed = contract(hot, tok_ref[...], 0, 0).astype(BF)
    packed_meta = contract(hot, meta, 0, 0).astype(BF)
    for index in range(GROUPS):
        out_refs[index][:, :features] = packed[index * share : (index + 1) * share]
        out_refs[index][:, features:] = packed_meta[index * share : (index + 1) * share]


def cot_pack_kernel(pieces, share, *refs):
    piece_refs, hot_ref = refs[:pieces], refs[pieces]
    out_refs, full_ref = refs[pieces + 1 : -1], refs[-1]
    me = lax.axis_index("tp")
    rows = hot_ref.shape[0]
    width = piece_refs[0].shape[1] // 2
    features = width * pieces

    def read(ref):
        gain = jnp.sum(ref[rows:, :width].astype(F32), axis=0, keepdims=True)
        return ref[:rows, width:].astype(F32), gain * ref[:rows, :width].astype(F32)

    square_sum = 0.0
    cross_sum = 0.0
    for ref in piece_refs:
        saved, scaled = read(ref)
        square_sum += jnp.sum(saved * saved, axis=1, keepdims=True)
        cross_sum += jnp.sum(saved * scaled, axis=1, keepdims=True)
    inv_rms = lax.rsqrt(square_sum / features + epsilon)
    factor = inv_rms * inv_rms * inv_rms * cross_sum / features
    for index, ref in enumerate(piece_refs):
        saved, scaled = read(ref)
        column = pl.multiple_of(jnp.bitwise_xor(me, index) * width, width)
        full_ref[:, pl.ds(column, width)] = (inv_rms * scaled - saved * factor).astype(BF)
    packed = contract(hot_ref[...], full_ref[...], 0, 0).astype(BF)
    for index in range(GROUPS):
        out_refs[index][...] = packed[index * share : (index + 1) * share]


def token_route_kernel(group_size, capacity, *refs):
    shifts = len(refs) - group_size - 3
    msg_refs, out_refs = refs[:shifts], refs[shifts : shifts + group_size]
    hot0_ref, hot1_ref, full_ref = refs[-3:]
    share, width = msg_refs[0].shape
    features = width - META
    slots = shifts * capacity
    _, mine = place(group_size)
    lower = strict_lower(share)
    gates = []
    for index, ref in enumerate(msg_refs):
        row = slice(index * share, (index + 1) * share)
        full_ref[row, :] = ref[:, :features]
        meta = ref[:, features:].astype(F32)
        gates.append((meta[:, 2:3], meta[:, 3:4]))
        experts = [meta[:, k : k + 1].astype(jnp.int32) - 1 for k in range(2)]
        members = [one_hot(e, META) for e in experts]
        before = contract(lower, members[0] + members[1], 1, 0)
        for expert, member, hot_ref in zip(experts, members, (hot0_ref, hot1_ref)):
            rank = jnp.sum(before * member.astype(F32), axis=1, keepdims=True)
            slot = jnp.bitwise_xor(expert, mine) * slots + index * capacity
            slot = jnp.where(expert < 0, -1, slot + rank.astype(jnp.int32))
            hot_ref[row, :] = one_hot(slot, group_size * slots)
    hot0, hot1 = hot0_ref[...], hot1_ref[...]
    total = shifts * share
    gate0 = lane_of((jnp.concatenate([g[0] for g in gates], axis=0),), total).astype(BF)
    gate1 = lane_of((jnp.concatenate([g[1] for g in gates], axis=0),), total).astype(BF)
    packed_gate = contract(hot0, gate0, 0, 0) + contract(hot1, gate1, 0, 0)
    packed = contract(hot0 + hot1, full_ref[...], 0, 0)
    for index in range(group_size):
        row = slice(index * slots, (index + 1) * slots)
        out_refs[index][:, :features] = packed[row].astype(BF)
        out_refs[index][:, features:] = packed_gate[row].astype(BF)


def cot_route_kernel(group_size, *refs):
    shifts = len(refs) - group_size - 3
    msg_refs, hot0_ref, hot1_ref = refs[:shifts], refs[shifts], refs[shifts + 1]
    out_refs, full_ref = refs[shifts + 2 : -1], refs[-1]
    share = msg_refs[0].shape[0]
    slots = hot0_ref.shape[1] // group_size
    for index, ref in enumerate(msg_refs):
        full_ref[index * share : (index + 1) * share, :] = ref[...]
    packed = contract(hot0_ref[...] + hot1_ref[...], full_ref[...], 0, 0)
    for index in range(group_size):
        out_refs[index][...] = packed[index * slots : (index + 1) * slots].astype(BF)


def combine_kernel(group_size, shifts, *refs):
    piece_refs, hot0_ref, hot1_ref = refs[:group_size], refs[group_size], refs[group_size + 1]
    out_refs = refs[group_size + 2 :]
    features = piece_refs[0].shape[1] - META
    share = hot0_ref.shape[0] // shifts
    rows = jnp.concatenate([ref[...].astype(F32) for ref in piece_refs], axis=0).astype(BF)
    hot0, hot1 = hot0_ref[...], hot1_ref[...]
    summed = contract(hot0 + hot1, rows[:, :features], 1, 0).astype(BF)
    grad0 = contract(hot0, rows[:, features:], 1, 0)[:, 0:1]
    grad1 = contract(hot1, rows[:, features:], 1, 0)[:, 0:1]
    meta = lane_of((grad0, grad1), shifts * share).astype(BF)
    for index in range(shifts):
        row = slice(index * share, (index + 1) * share)
        out_refs[index][:, :features] = summed[row]
        out_refs[index][:, features:] = meta[row]


def finish_kernel(hot_ref, *refs):
    msg_refs, tok_ref, gates_ref = refs[:GROUPS], refs[-2], refs[-1]
    features = tok_ref.shape[1]
    rows = jnp.concatenate([ref[...] for ref in msg_refs], axis=0)
    hot = hot_ref[...]
    tok_ref[...] = contract(hot, rows[:, :features], 1, 0).astype(BF)
    grads = contract(rows[:, features:].astype(F32).T.astype(BF), hot, 1, 1)
    gates_ref[...] = grads[0:2].astype(BF)


def forward_kernel(*refs):
    count = len(refs) - 6
    piece_refs, (gate_ref, up_ref) = refs[:count], refs[count : count + 2]
    rows_ref, meta_ref, pre_gate_ref, pre_up_ref = refs[count + 2 :]
    features = rows_ref.shape[1]

    @pl.when(pl.program_id(0) == 0)
    def _():
        first = 0
        for ref in piece_refs:
            last = first + ref.shape[0]
            rows_ref[first:last, :] = ref[:, :features]
            meta_ref[first:last, :] = ref[:, features:]
            first = last

    rows = rows_ref[...]
    pre_gate_ref[...] = contract(rows, gate_ref[0], 1, 0)
    pre_up_ref[...] = contract(rows, up_ref[0], 1, 0)


def backward_kernel(group_size, *refs):
    piece_refs = refs[:group_size]
    meta_ref, pre_gate_ref, pre_up_ref, gate_ref, up_ref, down_ref = refs[
        group_size : group_size + 6
    ]
    out_refs = refs[group_size + 6 : 2 * group_size + 6]
    d_gate_ref, d_up_ref, hidden_ref, scaled_ref, cot_ref, total_ref, grad_ref = refs[
        2 * group_size + 6 :
    ]
    step = pl.program_id(0)
    slots, features = piece_refs[0].shape
    rows = cot_ref.shape[0]
    weight = meta_ref[:, 0:1].astype(F32)

    @pl.when(step == 0)
    def _():
        for index, ref in enumerate(piece_refs):
            cot_ref[index * slots : (index + 1) * slots, :] = ref[...]
        scaled_ref[...] = (weight * cot_ref[...].astype(F32)).astype(BF)

    hid_grad = contract(cot_ref[...], down_ref[0], 1, 1)
    pre_gate, pre_up = pre_gate_ref[...], pre_up_ref[...]
    sigmoid_gate = jax.nn.sigmoid(pre_gate)
    activated = pre_gate * sigmoid_gate
    hidden = activated * pre_up
    grad = jnp.sum(hidden * hid_grad, axis=1, keepdims=True)
    d_hidden = weight * hid_grad
    d_gate = (d_hidden * pre_up * sigmoid_gate * (1.0 + pre_gate * (1.0 - sigmoid_gate))).astype(BF)
    d_up = (d_hidden * activated).astype(BF)
    d_gate_ref[...] = d_gate
    d_up_ref[...] = d_up
    hidden_ref[...] = hidden.astype(BF)
    back = contract(d_gate, gate_ref[0], 1, 1) + contract(d_up, up_ref[0], 1, 1)

    @pl.when(step == 0)
    def _():
        total_ref[...] = back
        grad_ref[...] = lane_of((grad,), rows)

    @pl.when(step > 0)
    def _():
        total_ref[...] += back
        grad_ref[...] += lane_of((grad,), rows)

    @pl.when(step == pl.num_programs(0) - 1)
    def _():
        for index, ref in enumerate(out_refs):
            row = slice(index * slots, (index + 1) * slots)
            ref[:, :features] = total_ref[row, :].astype(BF)
            ref[:, features:] = grad_ref[row, :].astype(BF)


def weight_kernel(sets, rows_ref, *refs):
    d_gate, d_up, hidden, scaled = (refs[k * sets : (k + 1) * sets] for k in range(4))
    grad_gate_ref, grad_up_ref, grad_down_ref, both_ref, turned_ref = refs[4 * sets :]
    hidden_width = hidden[0].shape[1]

    @pl.when(pl.program_id(0) == 0)
    def _():
        first = 0
        for gate, up, hid in zip(d_gate, d_up, hidden):
            last = first + gate.shape[0]
            both_ref[first:last, :hidden_width] = gate[...]
            both_ref[first:last, hidden_width:] = up[...]
            turned_ref[:, first:last] = hid[...].T
            first = last

    both = contract(rows_ref[...], both_ref[...], 0, 0)
    grad_gate_ref[0] = both[:, :hidden_width].astype(BF)
    grad_up_ref[0] = both[:, hidden_width:].astype(BF)
    cots = jnp.concatenate([ref[...] for ref in scaled], axis=0)
    grad_down_ref[0] = contract(turned_ref[...], cots, 1, 0).astype(BF)


def forward_call(pieces, w_gate, w_up):
    features, hidden = w_gate.shape[1:]
    rows = sum(p.shape[0] for p in pieces)
    tile = hidden // HIDDEN_TILES
    whole = lambda a: pl.BlockSpec(a.shape, lambda f: (0, 0))
    weight = pl.BlockSpec((1, features, tile), lambda f: (0, 0, f))
    return pl.pallas_call(
        forward_kernel,
        grid=(HIDDEN_TILES,),
        out_shape=[
            jax.ShapeDtypeStruct((rows, features), BF),
            jax.ShapeDtypeStruct((rows, META), BF),
            jax.ShapeDtypeStruct((rows, hidden), F32),
            jax.ShapeDtypeStruct((rows, hidden), F32),
        ],
        in_specs=[whole(p) for p in pieces] + [weight, weight],
        out_specs=[
            pl.BlockSpec((rows, features), lambda f: (0, 0)),
            pl.BlockSpec((rows, META), lambda f: (0, 0)),
            pl.BlockSpec((rows, tile), lambda f: (0, f)),
            pl.BlockSpec((rows, tile), lambda f: (0, f)),
        ],
        compiler_params=pltpu.CompilerParams(vmem_limit_bytes=BIG_VMEM),
        cost_estimate=pl.CostEstimate(
            flops=4 * rows * features * hidden,
            bytes_accessed=4 * features * hidden + 4 * rows * features + 8 * rows * hidden,
            transcendentals=0,
        ),
    )(*pieces, w_gate, w_up)


def backward_call(index, pieces, meta, pre_gate, pre_up, w_gate, w_up, w_down):
    features, hidden = w_gate.shape[1:]
    slots = pieces[0].shape[0]
    rows = slots * len(pieces)
    tile = hidden // HIDDEN_TILES
    whole = lambda shape: pl.BlockSpec(shape, lambda f: (0, 0))
    weight = pl.BlockSpec((1, features, tile), lambda f: (0, 0, f))
    held = pl.BlockSpec((rows, tile), lambda f: (index, f))
    kept = pl.BlockSpec((rows, tile), lambda f: (0, f))
    result = pl.pallas_call(
        functools.partial(backward_kernel, len(pieces)),
        grid=(HIDDEN_TILES,),
        out_shape=[jax.ShapeDtypeStruct((slots, features + META), BF)] * len(pieces)
        + [jax.ShapeDtypeStruct((rows, hidden), BF)] * 3
        + [jax.ShapeDtypeStruct((rows, features), BF)],
        in_specs=[whole(p.shape) for p in pieces]
        + [pl.BlockSpec((rows, META), lambda f: (index, 0)), held, held, weight, weight]
        + [pl.BlockSpec((1, tile, features), lambda f: (0, f, 0))],
        out_specs=[whole((slots, features + META))] * len(pieces)
        + [kept] * 3
        + [whole((rows, features))],
        scratch_shapes=[
            pltpu.VMEM((rows, features), BF),
            pltpu.VMEM((rows, features), F32),
            pltpu.VMEM((rows, META), F32),
        ],
        compiler_params=pltpu.CompilerParams(vmem_limit_bytes=BIG_VMEM),
        cost_estimate=pl.CostEstimate(
            flops=6 * rows * features * hidden,
            bytes_accessed=6 * features * hidden + 6 * rows * features + 14 * rows * hidden,
            transcendentals=rows * hidden,
        ),
    )(*pieces, meta, pre_gate, pre_up, w_gate, w_up, w_down)
    return result[: len(pieces)], result[len(pieces) :]


def weight_call(rows, kept):
    d_gate, d_up, hidden, scaled = ([k[i] for k in kept] for i in range(4))
    total, features = rows.shape
    width = hidden[0].shape[1]
    tile = features // FEATURE_TILES
    whole = lambda a: pl.BlockSpec(a.shape, lambda d: (0, 0))
    return pl.pallas_call(
        functools.partial(weight_kernel, len(kept)),
        grid=(FEATURE_TILES,),
        out_shape=[
            jax.ShapeDtypeStruct((1, features, width), BF),
            jax.ShapeDtypeStruct((1, features, width), BF),
            jax.ShapeDtypeStruct((1, width, features), BF),
        ],
        in_specs=[pl.BlockSpec((total, tile), lambda d: (0, d))]
        + [whole(a) for a in (*d_gate, *d_up, *hidden)]
        + [pl.BlockSpec((a.shape[0], tile), lambda d: (0, d)) for a in scaled],
        out_specs=[
            pl.BlockSpec((1, tile, width), lambda d: (0, d, 0)),
            pl.BlockSpec((1, tile, width), lambda d: (0, d, 0)),
            pl.BlockSpec((1, width, tile), lambda d: (0, 0, d)),
        ],
        scratch_shapes=[pltpu.VMEM((total, 2 * width), BF), pltpu.VMEM((width, total), BF)],
        compiler_params=pltpu.CompilerParams(vmem_limit_bytes=BIG_VMEM),
        cost_estimate=pl.CostEstimate(
            flops=6 * total * features * width,
            bytes_accessed=6 * features * width + 4 * total * features + 6 * total * width,
            transcendentals=0,
        ),
    )(rows, *d_gate, *d_up, *hidden, *scaled)


def call(kernel, outs, args, scratch=(), flops=0):
    outs = [jax.ShapeDtypeStruct(shape, BF) for shape in outs]
    size = sum(a.size * a.dtype.itemsize for a in args) + sum(o.size * 2 for o in outs)
    return pl.pallas_call(
        kernel,
        out_shape=outs,
        in_specs=[pl.BlockSpec(memory_space=pltpu.VMEM)] * len(args),
        out_specs=[pl.BlockSpec(memory_space=pltpu.VMEM)] * len(outs),
        scratch_shapes=[pltpu.VMEM(shape, dtype) for shape, dtype in scratch],
        compiler_params=pltpu.CompilerParams(vmem_limit_bytes=SMALL_VMEM),
        cost_estimate=pl.CostEstimate(flops=flops, bytes_accessed=size, transcendentals=0),
    )(*args)


def local(tokens, routes, gates, w_gate, w_up, w_down, moe_out, norm_gain, out_grad):
    devices = lax.axis_size(AXES)
    pieces = lax.axis_size("tp")
    group_size = devices // GROUPS
    tok_rows, features = tokens.shape
    capacity = 4 * tok_rows // devices
    share = 3 * tok_rows // 8
    wide = features + META

    def over_tp(array, bits):
        pairs = [(d, d ^ bits) for d in range(pieces)]
        return lax.ppermute(array, "tp", pairs)

    def over_plane(array, bits):
        pairs = [
            (d, d // group_size * group_size + (d % group_size ^ bits)) for d in range(devices)
        ]
        return lax.ppermute(array, AXES, pairs)

    def over_z(array, shift):
        pairs = [(d, (d + shift * group_size) % devices) for d in range(devices)]
        return lax.ppermute(array, AXES, pairs)

    part = [(tok_rows + GAIN_ROWS, 2 * moe_out.shape[1])] * pieces
    split = call(
        functools.partial(split_kernel, pieces), part, (moe_out, norm_gain[None, :], out_grad)
    )
    *tok_msgs, hot = call(
        functools.partial(token_pack_kernel, group_size, share),
        [(share, wide)] * GROUPS + [(tok_rows, GROUPS * share)],
        (tokens, routes.T, gates.T),
        scratch=[((8, tok_rows), F32)],
        flops=2 * tok_rows * GROUPS * share * wide,
    )
    split = [split[0]] + [over_tp(split[m], m) for m in range(1, pieces)]
    order = [s for group in SETS for s in group]
    tok_at = {s: over_z(tok_msgs[s], s) if s else tok_msgs[s] for s in order}
    cot_msgs = call(
        functools.partial(cot_pack_kernel, pieces, share),
        [(share, features)] * GROUPS,
        (*split, hot),
        scratch=[((tok_rows, features), BF)],
        flops=2 * tok_rows * GROUPS * share * features,
    )
    cot_at = {s: over_z(cot_msgs[s], s) if s else cot_msgs[s] for s in order}

    hots, tok_in, cot_in = [], [], []
    for group in SETS:
        count = len(group)
        slots = count * capacity
        *out, hot0, hot1 = call(
            functools.partial(token_route_kernel, group_size, capacity),
            [(slots, wide)] * group_size + [(count * share, group_size * slots)] * 2,
            [tok_at[s] for s in group],
            scratch=[((count * share, features), BF)],
            flops=2 * count * share * group_size * slots * wide,
        )
        hots.append((hot0, hot1))
        tok_in.append([out[0]] + [over_plane(out[m], m) for m in range(1, group_size)])
    for group, (hot0, hot1) in zip(SETS, hots):
        count = len(group)
        slots = count * capacity
        out = call(
            functools.partial(cot_route_kernel, group_size),
            [(slots, features)] * group_size,
            [cot_at[s] for s in group] + [hot0, hot1],
            scratch=[((count * share, features), BF)],
            flops=2 * count * share * group_size * slots * features,
        )
        cot_in.append([out[0]] + [over_plane(out[m], m) for m in range(1, group_size)])

    row_block, meta, pre_gate, pre_up = forward_call([p for t in tok_in for p in t], w_gate, w_up)
    backs, kept = [], []
    for index, cots in enumerate(cot_in):
        back, keep = backward_call(index, cots, meta, pre_gate, pre_up, w_gate, w_up, w_down)
        backs.append([back[0]] + [over_plane(back[m], m) for m in range(1, group_size)])
        kept.append(keep)
    grad_gate, grad_up, grad_down = weight_call(row_block, kept)

    home = {}
    for group, back, (hot0, hot1) in zip(SETS, backs, hots):
        count = len(group)
        out = call(
            functools.partial(combine_kernel, group_size, count),
            [(share, wide)] * count,
            [*back, hot0, hot1],
            flops=2 * hot0.size * wide,
        )
        for s, array in zip(group, out):
            home[s] = over_z(array, -s) if s else array
    token_grad, gates_grad = call(
        finish_kernel,
        [(tok_rows, features), (routes.shape[1], tok_rows)],
        [hot] + [home[s] for s in range(GROUPS)],
        flops=2 * hot.size * wide,
    )
    return (token_grad, gates_grad.T, grad_gate, grad_up, grad_down)


def solution(mesh):
    in_specs = (
        P(AXES, None),
        P(AXES, None),
        P(AXES, None),
        P(AXES, None, None),
        P(AXES, None, None),
        P(AXES, None, None),
        P("ep", "tp"),
        P("tp"),
        P("ep", "tp"),
    )
    out_specs = (
        P(AXES, None),
        P(AXES, None),
        P(AXES, None, None),
        P(AXES, None, None),
        P(AXES, None, None),
    )
    return jax.shard_map(local, mesh=mesh, in_specs=in_specs, out_specs=out_specs, check_vma=False)
```

```python
import functools

import jax
import jax.numpy as jnp
from jax import lax
from jax.experimental import pallas as pl
from jax.experimental.pallas import tpu as pltpu
from jax.sharding import PartitionSpec as P


epsilon = 1e-06
AXES = ("ep", "tp")
GROUPS = 4
META = 128
GAIN_ROWS = 16
FEATURE_TILES = 4
SMALL_VMEM = 16 * 2**20
BIG_VMEM = 24 * 2**20
SETS = ((1, 2), (3, 0))
TOKEN_SHIFTS = (3, 1, 2)
COT_SHIFTS = (1, 2, 3)
BF = jnp.bfloat16
F32 = jnp.float32


def contract(left, right, left_dim, right_dim):
    return lax.dot_general(
        left, right, (((left_dim,), (right_dim,)), ((), ())), preferred_element_type=F32
    )


def one_hot(column, width):
    lanes = lax.broadcasted_iota(jnp.int32, (column.shape[0], width), 1)
    return jnp.where(column == lanes, 1.0, 0.0).astype(BF)


def strict_lower(rows):
    above = lax.broadcasted_iota(jnp.int32, (rows, rows), 1)
    below = lax.broadcasted_iota(jnp.int32, (rows, rows), 0)
    return jnp.where(above < below, 1.0, 0.0).astype(BF)


def lane_of(column_values, rows):
    lanes = lax.broadcasted_iota(jnp.int32, (rows, META), 1)
    result = jnp.zeros((rows, META), F32)
    for lane, column in enumerate(column_values):
        result = jnp.where(lanes == lane, column, result)
    return result


def place(group_size):
    flat = lax.axis_index("ep") * lax.axis_size("tp") + lax.axis_index("tp")
    return lax.div(flat, group_size), lax.rem(flat, group_size)


def split_kernel(pieces, moe_ref, gain_ref, grad_ref, *out_refs):
    me = lax.axis_index("tp")
    width = moe_ref.shape[1]
    rows = moe_ref.shape[0] // pieces
    gain = gain_ref[...]
    high = gain.astype(BF).astype(F32)
    middle = (gain - high).astype(BF).astype(F32)
    low = gain - high - middle
    line = lax.broadcasted_iota(jnp.int32, (GAIN_ROWS, width), 0)
    parts = jnp.where(line == 0, high, jnp.where(line == 1, middle, 0.0))
    parts = jnp.where(line == 2, low, parts).astype(BF)
    for index in range(pieces):
        first = pl.multiple_of(jnp.bitwise_xor(me, index) * rows, rows)
        out_refs[index][:rows, :width] = grad_ref[pl.ds(first, rows), :]
        out_refs[index][:rows, width:] = moe_ref[pl.ds(first, rows), :]
        out_refs[index][rows:, :width] = parts
        out_refs[index][rows:, width:] = jnp.zeros((GAIN_ROWS, width), BF)


def token_pack_kernel(group_size, share, tok_ref, routes_ref, gates_ref, *refs):
    out_refs, hot_ref, rows_ref = refs[:-2], refs[-2], refs[-1]
    rows, features = tok_ref.shape
    plane, _ = place(group_size)
    rows_ref[...] = jnp.zeros_like(rows_ref)
    rows_ref[0:2, :] = routes_ref[...].astype(F32)
    rows_ref[2:4, :] = gates_ref[...]
    unit_row = lax.broadcasted_iota(jnp.int32, (rows, rows), 0)
    unit_col = lax.broadcasted_iota(jnp.int32, (rows, rows), 1)
    unit = jnp.where(unit_row == unit_col, 1.0, 0.0).astype(BF)
    columns = contract(unit, rows_ref[...].astype(BF), 1, 1)
    first = columns[:, 0:1].astype(jnp.int32)
    second = columns[:, 1:2].astype(jnp.int32)
    group = lax.div(first, group_size)
    shift = lax.rem(group - plane + GROUPS, GROUPS)
    member = one_hot(shift, META)
    before = contract(strict_lower(rows), member, 1, 0)
    rank = jnp.sum(before * member.astype(F32), axis=1, keepdims=True).astype(jnp.int32)
    hot = one_hot(shift * share + rank, GROUPS * share)
    hot_ref[...] = hot
    base = group * group_size
    meta = lane_of(
        (
            (first - base + 1).astype(F32),
            (second - base + 1).astype(F32),
            columns[:, 2:3],
            columns[:, 3:4],
        ),
        rows,
    ).astype(BF)
    packed = contract(hot, tok_ref[...], 0, 0).astype(BF)
    packed_meta = contract(hot, meta, 0, 0).astype(BF)
    for index in range(GROUPS):
        out_refs[index][:, :features] = packed[index * share : (index + 1) * share]
        out_refs[index][:, features:] = packed_meta[index * share : (index + 1) * share]


def cot_pack_kernel(pieces, share, *refs):
    piece_refs, hot_ref = refs[:pieces], refs[pieces]
    out_refs, full_ref = refs[pieces + 1 : -1], refs[-1]
    me = lax.axis_index("tp")
    rows = hot_ref.shape[0]
    width = piece_refs[0].shape[1] // 2
    features = width * pieces

    def read(ref):
        gain = jnp.sum(ref[rows:, :width].astype(F32), axis=0, keepdims=True)
        return ref[:rows, width:].astype(F32), gain * ref[:rows, :width].astype(F32)

    square_sum = 0.0
    cross_sum = 0.0
    for ref in piece_refs:
        saved, scaled = read(ref)
        square_sum += jnp.sum(saved * saved, axis=1, keepdims=True)
        cross_sum += jnp.sum(saved * scaled, axis=1, keepdims=True)
    inv_rms = lax.rsqrt(square_sum / features + epsilon)
    factor = inv_rms * inv_rms * inv_rms * cross_sum / features
    for index, ref in enumerate(piece_refs):
        saved, scaled = read(ref)
        column = pl.multiple_of(jnp.bitwise_xor(me, index) * width, width)
        full_ref[:, pl.ds(column, width)] = (inv_rms * scaled - saved * factor).astype(BF)
    packed = contract(hot_ref[...], full_ref[...], 0, 0).astype(BF)
    for index in range(GROUPS):
        out_refs[index][...] = packed[index * share : (index + 1) * share]


def token_route_kernel(group_size, capacity, *refs):
    shifts = len(refs) - group_size - 3
    msg_refs, out_refs = refs[:shifts], refs[shifts : shifts + group_size]
    hot0_ref, hot1_ref, full_ref = refs[-3:]
    share, width = msg_refs[0].shape
    features = width - META
    slots = shifts * capacity
    _, mine = place(group_size)
    lower = strict_lower(share)
    gates = []
    for index, ref in enumerate(msg_refs):
        row = slice(index * share, (index + 1) * share)
        full_ref[row, :] = ref[:, :features]
        meta = ref[:, features:].astype(F32)
        gates.append((meta[:, 2:3], meta[:, 3:4]))
        experts = [meta[:, k : k + 1].astype(jnp.int32) - 1 for k in range(2)]
        members = [one_hot(e, META) for e in experts]
        before = contract(lower, members[0] + members[1], 1, 0)
        for expert, member, hot_ref in zip(experts, members, (hot0_ref, hot1_ref)):
            rank = jnp.sum(before * member.astype(F32), axis=1, keepdims=True)
            slot = jnp.bitwise_xor(expert, mine) * slots + index * capacity
            slot = jnp.where(expert < 0, -1, slot + rank.astype(jnp.int32))
            hot_ref[row, :] = one_hot(slot, group_size * slots)
    hot0, hot1 = hot0_ref[...], hot1_ref[...]
    total = shifts * share
    gate0 = lane_of((jnp.concatenate([g[0] for g in gates], axis=0),), total).astype(BF)
    gate1 = lane_of((jnp.concatenate([g[1] for g in gates], axis=0),), total).astype(BF)
    packed_gate = contract(hot0, gate0, 0, 0) + contract(hot1, gate1, 0, 0)
    packed = contract(hot0 + hot1, full_ref[...], 0, 0)
    for index in range(group_size):
        row = slice(index * slots, (index + 1) * slots)
        out_refs[index][:, :features] = packed[row].astype(BF)
        out_refs[index][:, features:] = packed_gate[row].astype(BF)


def cot_route_kernel(group_size, *refs):
    shifts = len(refs) - group_size - 3
    msg_refs, hot0_ref, hot1_ref = refs[:shifts], refs[shifts], refs[shifts + 1]
    out_refs, full_ref = refs[shifts + 2 : -1], refs[-1]
    share = msg_refs[0].shape[0]
    slots = hot0_ref.shape[1] // group_size
    for index, ref in enumerate(msg_refs):
        full_ref[index * share : (index + 1) * share, :] = ref[...]
    packed = contract(hot0_ref[...] + hot1_ref[...], full_ref[...], 0, 0)
    for index in range(group_size):
        out_refs[index][...] = packed[index * slots : (index + 1) * slots].astype(BF)


def combine_kernel(group_size, shifts, *refs):
    piece_refs, hot0_ref, hot1_ref = refs[:group_size], refs[group_size], refs[group_size + 1]
    out_refs = refs[group_size + 2 :]
    features = piece_refs[0].shape[1] - META
    share = hot0_ref.shape[0] // shifts
    rows = jnp.concatenate([ref[...].astype(F32) for ref in piece_refs], axis=0).astype(BF)
    hot0, hot1 = hot0_ref[...], hot1_ref[...]
    summed = contract(hot0 + hot1, rows[:, :features], 1, 0).astype(BF)
    grad0 = contract(hot0, rows[:, features:], 1, 0)[:, 0:1]
    grad1 = contract(hot1, rows[:, features:], 1, 0)[:, 0:1]
    meta = lane_of((grad0, grad1), shifts * share).astype(BF)
    for index in range(shifts):
        row = slice(index * share, (index + 1) * share)
        out_refs[index][:, :features] = summed[row]
        out_refs[index][:, features:] = meta[row]


def finish_kernel(hot_ref, *refs):
    msg_refs, tok_ref, gates_ref = refs[:GROUPS], refs[-2], refs[-1]
    features = tok_ref.shape[1]
    rows = jnp.concatenate([ref[...] for ref in msg_refs], axis=0)
    hot = hot_ref[...]
    tok_ref[...] = contract(hot, rows[:, :features], 1, 0).astype(BF)
    grads = contract(rows[:, features:].astype(F32).T.astype(BF), hot, 1, 1)
    gates_ref[...] = grads[0:2].astype(BF)


def forward_kernel(*refs):
    count = len(refs) - 6
    piece_refs, (gate_ref, up_ref) = refs[:count], refs[count : count + 2]
    rows_ref, meta_ref, pre_gate_ref, pre_up_ref = refs[count + 2 :]
    features = rows_ref.shape[1]
    first = 0
    for ref in piece_refs:
        last = first + ref.shape[0]
        rows_ref[first:last, :] = ref[:, :features]
        meta_ref[first:last, :] = ref[:, features:]
        first = last
    rows = rows_ref[...]
    pre_gate_ref[...] = contract(rows, gate_ref[0], 1, 0)
    pre_up_ref[...] = contract(rows, up_ref[0], 1, 0)


def backward_kernel(group_size, first, *refs):
    piece_refs = refs[:group_size]
    meta_ref, pre_gate_ref, pre_up_ref, gate_ref, up_ref, down_ref = refs[
        group_size : group_size + 6
    ]
    out_refs = refs[group_size + 6 : 2 * group_size + 6]
    d_gate_ref, d_up_ref, hidden_ref, scaled_ref, cot_ref = refs[2 * group_size + 6 :]
    slots, features = piece_refs[0].shape
    rows = cot_ref.shape[0]
    held = slice(first, first + rows)
    for index, ref in enumerate(piece_refs):
        cot_ref[index * slots : (index + 1) * slots, :] = ref[...]
    weight = meta_ref[held, 0:1].astype(F32)
    hid_grad = contract(cot_ref[...], down_ref[0], 1, 1)
    pre_gate, pre_up = pre_gate_ref[held, :], pre_up_ref[held, :]
    sigmoid_gate = jax.nn.sigmoid(pre_gate)
    activated = pre_gate * sigmoid_gate
    hidden = activated * pre_up
    grad = lane_of((jnp.sum(hidden * hid_grad, axis=1, keepdims=True),), rows).astype(BF)
    d_hidden = weight * hid_grad
    d_gate_ref[...] = (
        d_hidden * pre_up * sigmoid_gate * (1.0 + pre_gate * (1.0 - sigmoid_gate))
    ).astype(BF)
    d_up_ref[...] = (d_hidden * activated).astype(BF)
    hidden_ref[...] = hidden.astype(BF)
    tile = features // FEATURE_TILES
    for start in range(0, features, tile):
        column = slice(start, start + tile)
        back = contract(d_gate_ref[...], gate_ref[0, column, :], 1, 1)
        back = (back + contract(d_up_ref[...], up_ref[0, column, :], 1, 1)).astype(BF)
        for index, ref in enumerate(out_refs):
            ref[:, column] = back[index * slots : (index + 1) * slots]
    for index, ref in enumerate(out_refs):
        ref[:, features:] = grad[index * slots : (index + 1) * slots]
    scaled_ref[...] = (weight * cot_ref[...].astype(F32)).astype(BF)


def weight_kernel(sets, rows_ref, *refs):
    d_gate, d_up, hidden, scaled = (refs[k * sets : (k + 1) * sets] for k in range(4))
    grad_gate_ref, grad_up_ref, grad_down_ref, both_ref, turned_ref = refs[4 * sets :]
    hidden_width = hidden[0].shape[1]

    @pl.when(pl.program_id(0) == 0)
    def _():
        first = 0
        for gate, up, hid in zip(d_gate, d_up, hidden):
            last = first + gate.shape[0]
            both_ref[first:last, :hidden_width] = gate[...]
            both_ref[first:last, hidden_width:] = up[...]
            turned_ref[:, first:last] = hid[...].T
            first = last

    both = contract(rows_ref[...], both_ref[...], 0, 0)
    grad_gate_ref[0] = both[:, :hidden_width].astype(BF)
    grad_up_ref[0] = both[:, hidden_width:].astype(BF)
    cots = jnp.concatenate([ref[...] for ref in scaled], axis=0)
    grad_down_ref[0] = contract(turned_ref[...], cots, 1, 0).astype(BF)


def forward_call(pieces, w_gate, w_up):
    features, hidden = w_gate.shape[1:]
    rows = sum(p.shape[0] for p in pieces)
    return call(
        forward_kernel,
        [(rows, features), (rows, META), (rows, hidden, F32), (rows, hidden, F32)],
        [*pieces, w_gate, w_up],
        flops=4 * rows * features * hidden,
        limit=BIG_VMEM,
    )


def backward_call(first, pieces, *held):
    features, hidden = held[3].shape[1:]
    slots = pieces[0].shape[0]
    rows = slots * len(pieces)
    result = call(
        functools.partial(backward_kernel, len(pieces), first),
        [(slots, features + META)] * len(pieces) + [(rows, hidden)] * 3 + [(rows, features)],
        [*pieces, *held],
        scratch=[((rows, features), BF)],
        flops=6 * rows * features * hidden,
        limit=BIG_VMEM,
    )
    return result[: len(pieces)], result[len(pieces) :]


def weight_call(rows, kept):
    d_gate, d_up, hidden, scaled = ([k[i] for k in kept] for i in range(4))
    total, features = rows.shape
    width = hidden[0].shape[1]
    tile = features // FEATURE_TILES
    whole = lambda a: pl.BlockSpec(a.shape, lambda d: (0, 0))
    return pl.pallas_call(
        functools.partial(weight_kernel, len(kept)),
        grid=(FEATURE_TILES,),
        out_shape=[
            jax.ShapeDtypeStruct((1, features, width), BF),
            jax.ShapeDtypeStruct((1, features, width), BF),
            jax.ShapeDtypeStruct((1, width, features), BF),
        ],
        in_specs=[pl.BlockSpec((total, tile), lambda d: (0, d))]
        + [whole(a) for a in (*d_gate, *d_up, *hidden)]
        + [pl.BlockSpec((a.shape[0], tile), lambda d: (0, d)) for a in scaled],
        out_specs=[
            pl.BlockSpec((1, tile, width), lambda d: (0, d, 0)),
            pl.BlockSpec((1, tile, width), lambda d: (0, d, 0)),
            pl.BlockSpec((1, width, tile), lambda d: (0, 0, d)),
        ],
        scratch_shapes=[pltpu.VMEM((total, 2 * width), BF), pltpu.VMEM((width, total), BF)],
        compiler_params=pltpu.CompilerParams(vmem_limit_bytes=BIG_VMEM),
        cost_estimate=pl.CostEstimate(
            flops=6 * total * features * width,
            bytes_accessed=6 * features * width + 4 * total * features + 6 * total * width,
            transcendentals=0,
        ),
    )(rows, *d_gate, *d_up, *hidden, *scaled)


def call(kernel, outs, args, scratch=(), flops=0, limit=SMALL_VMEM):
    outs = [jax.ShapeDtypeStruct(o[:2], o[2] if len(o) > 2 else BF) for o in outs]
    size = sum(a.size * a.dtype.itemsize for a in (*args, *outs))
    return pl.pallas_call(
        kernel,
        out_shape=outs,
        in_specs=[pl.BlockSpec(memory_space=pltpu.VMEM)] * len(args),
        out_specs=[pl.BlockSpec(memory_space=pltpu.VMEM)] * len(outs),
        scratch_shapes=[pltpu.VMEM(shape, dtype) for shape, dtype in scratch],
        compiler_params=pltpu.CompilerParams(vmem_limit_bytes=limit),
        cost_estimate=pl.CostEstimate(flops=flops, bytes_accessed=size, transcendentals=0),
    )(*args)


def local(tokens, routes, gates, w_gate, w_up, w_down, moe_out, norm_gain, out_grad):
    devices = lax.axis_size(AXES)
    pieces = lax.axis_size("tp")
    group_size = devices // GROUPS
    tok_rows, features = tokens.shape
    capacity = 4 * tok_rows // devices
    share = 3 * tok_rows // 8
    wide = features + META

    def over_tp(array, bits):
        pairs = [(d, d ^ bits) for d in range(pieces)]
        return lax.ppermute(array, "tp", pairs)

    def over_plane(array, bits):
        pairs = [
            (d, d // group_size * group_size + (d % group_size ^ bits)) for d in range(devices)
        ]
        return lax.ppermute(array, AXES, pairs)

    def over_z(array, shift):
        pairs = [(d, (d + shift * group_size) % devices) for d in range(devices)]
        return lax.ppermute(array, AXES, pairs)

    part = [(tok_rows + GAIN_ROWS, 2 * moe_out.shape[1])] * pieces
    *tok_msgs, hot = call(
        functools.partial(token_pack_kernel, group_size, share),
        [(share, wide)] * GROUPS + [(tok_rows, GROUPS * share)],
        (tokens, routes.T, gates.T),
        scratch=[((8, tok_rows), F32)],
        flops=2 * tok_rows * GROUPS * share * wide,
    )
    tok_at = {0: tok_msgs[0]}
    for s in TOKEN_SHIFTS:
        tok_at[s] = over_z(tok_msgs[s], s)
    split = call(
        functools.partial(split_kernel, pieces), part, (moe_out, norm_gain[None, :], out_grad)
    )
    split = [split[0]] + [over_tp(split[m], m) for m in range(1, pieces)]
    cot_msgs = call(
        functools.partial(cot_pack_kernel, pieces, share),
        [(share, features)] * GROUPS,
        (*split, hot),
        scratch=[((tok_rows, features), BF)],
        flops=2 * tok_rows * GROUPS * share * features,
    )
    cot_at = {0: cot_msgs[0]}
    for s in COT_SHIFTS:
        cot_at[s] = over_z(cot_msgs[s], s)

    hots, tok_in, cot_in = [], [], []
    for group in SETS:
        count = len(group)
        slots = count * capacity
        *out, hot0, hot1 = call(
            functools.partial(token_route_kernel, group_size, capacity),
            [(slots, wide)] * group_size + [(count * share, group_size * slots)] * 2,
            [tok_at[s] for s in group],
            scratch=[((count * share, features), BF)],
            flops=2 * count * share * group_size * slots * wide,
        )
        hots.append((hot0, hot1))
        tok_in.append([out[0]] + [over_plane(out[m], m) for m in range(1, group_size)])
    for group, (hot0, hot1) in zip(SETS, hots):
        count = len(group)
        slots = count * capacity
        out = call(
            functools.partial(cot_route_kernel, group_size),
            [(slots, features)] * group_size,
            [cot_at[s] for s in group] + [hot0, hot1],
            scratch=[((count * share, features), BF)],
            flops=2 * count * share * group_size * slots * features,
        )
        cot_in.append([out[0]] + [over_plane(out[m], m) for m in range(1, group_size)])

    row_block, meta, pre_gate, pre_up = forward_call([p for t in tok_in for p in t], w_gate, w_up)
    backs, kept, first = [], [], 0
    for cots in cot_in:
        back, keep = backward_call(first, cots, meta, pre_gate, pre_up, w_gate, w_up, w_down)
        first += cots[0].shape[0] * group_size
        backs.append([back[0]] + [over_plane(back[m], m) for m in range(1, group_size)])
        kept.append(keep)
    grad_gate, grad_up, grad_down = weight_call(row_block, kept)

    home = {}
    for group, back, (hot0, hot1) in zip(SETS, backs, hots):
        count = len(group)
        out = call(
            functools.partial(combine_kernel, group_size, count),
            [(share, wide)] * count,
            [*back, hot0, hot1],
            flops=2 * hot0.size * wide,
        )
        for s, array in zip(group, out):
            home[s] = over_z(array, -s) if s else array
    token_grad, gates_grad = call(
        finish_kernel,
        [(tok_rows, features), (routes.shape[1], tok_rows)],
        [hot] + [home[s] for s in range(GROUPS)],
        flops=2 * hot.size * wide,
    )
    return (token_grad, gates_grad.T, grad_gate, grad_up, grad_down)


def solution(mesh):
    in_specs = (
        P(AXES, None),
        P(AXES, None),
        P(AXES, None),
        P(AXES, None, None),
        P(AXES, None, None),
        P(AXES, None, None),
        P("ep", "tp"),
        P("tp"),
        P("ep", "tp"),
    )
    out_specs = (
        P(AXES, None),
        P(AXES, None),
        P(AXES, None, None),
        P(AXES, None, None),
        P(AXES, None, None),
    )

    return jax.shard_map(local, mesh=mesh, in_specs=in_specs, out_specs=out_specs, check_vma=False)
```

```python
import functools

import jax
import jax.numpy as jnp
from jax import lax
from jax.experimental import pallas as pl
from jax.experimental.pallas import tpu as pltpu
from jax.sharding import PartitionSpec as P


epsilon = 1e-06
AXES = ("ep", "tp")
GROUPS = 4
META = 128
GAIN_ROWS = 16
FEATURE_TILES = 4
SMALL_VMEM = 16 * 2**20
BIG_VMEM = 24 * 2**20
HEAD_VMEM = 60 * 2**20
TOKEN_SETS = ((3, 0), (1, 2))
SETS = ((1, 2), (3, 0))
TOKEN_SHIFTS = (3, 1, 2)
COT_SHIFTS = (1, 2, 3)
BF = jnp.bfloat16
F32 = jnp.float32


def contract(left, right, left_dim, right_dim):
    return lax.dot_general(
        left, right, (((left_dim,), (right_dim,)), ((), ())), preferred_element_type=F32
    )


def one_hot(column, width):
    lanes = lax.broadcasted_iota(jnp.int32, (column.shape[0], width), 1)
    return jnp.where(column == lanes, 1.0, 0.0).astype(BF)


def strict_lower(rows):
    above = lax.broadcasted_iota(jnp.int32, (rows, rows), 1)
    below = lax.broadcasted_iota(jnp.int32, (rows, rows), 0)
    return jnp.where(above < below, 1.0, 0.0).astype(BF)


def lane_of(column_values, rows):
    lanes = lax.broadcasted_iota(jnp.int32, (rows, META), 1)
    result = jnp.zeros((rows, META), F32)
    for lane, column in enumerate(column_values):
        result = jnp.where(lanes == lane, column, result)
    return result


def place(group_size):
    flat = lax.axis_index("ep") * lax.axis_size("tp") + lax.axis_index("tp")
    return lax.div(flat, group_size), lax.rem(flat, group_size)


def head_kernel(pieces, group_size, share, *refs):
    tok_hbm, routes_hbm, gates_hbm, moe_hbm, gain_hbm, grad_hbm = refs[:6]
    part_refs, refs = refs[6 : 6 + pieces], refs[6 + pieces :]
    out_refs, hot_ref = refs[:GROUPS], refs[GROUPS]
    tok_ref, routes_ref, gates_ref, gain_ref, lines_ref, sems = refs[GROUPS + 1 :]
    rows, features = tok_ref.shape
    width = moe_hbm.shape[1]
    me = lax.axis_index("tp")
    plane, _ = place(group_size)

    sources = [
        (routes_hbm, routes_ref),
        (gates_hbm, gates_ref),
        (tok_hbm, tok_ref),
        (gain_hbm, gain_ref),
    ]
    for index, ref in enumerate(part_refs):
        block = pl.ds(pl.multiple_of(jnp.bitwise_xor(me, index) * rows, rows), rows)
        sources.append((grad_hbm.at[block, :], ref.at[pl.ds(0, rows), pl.ds(0, width)]))
        sources.append((moe_hbm.at[block, :], ref.at[pl.ds(0, rows), pl.ds(width, width)]))
    copies = [pltpu.make_async_copy(a, b, sems.at[i]) for i, (a, b) in enumerate(sources)]
    for copy in copies:
        copy.start()

    lines_ref[...] = jnp.zeros_like(lines_ref)
    copies[0].wait()
    copies[1].wait()
    lines_ref[0:2, :] = routes_ref[...].astype(F32)
    lines_ref[2:4, :] = gates_ref[...]
    unit_row = lax.broadcasted_iota(jnp.int32, (rows, rows), 0)
    unit_col = lax.broadcasted_iota(jnp.int32, (rows, rows), 1)
    unit = jnp.where(unit_row == unit_col, 1.0, 0.0).astype(BF)
    columns = contract(unit, lines_ref[...].astype(BF), 1, 1)
    first = columns[:, 0:1].astype(jnp.int32)
    second = columns[:, 1:2].astype(jnp.int32)
    group = lax.div(first, group_size)
    shift = lax.rem(group - plane + GROUPS, GROUPS)
    member = one_hot(shift, META)
    before = contract(strict_lower(rows), member, 1, 0)
    rank = jnp.sum(before * member.astype(F32), axis=1, keepdims=True).astype(jnp.int32)
    hot = one_hot(shift * share + rank, GROUPS * share)
    hot_ref[...] = hot
    base = group * group_size
    meta = lane_of(
        (
            (first - base + 1).astype(F32),
            (second - base + 1).astype(F32),
            columns[:, 2:3],
            columns[:, 3:4],
        ),
        rows,
    ).astype(BF)
    packed_meta = contract(hot, meta, 0, 0).astype(BF)
    copies[2].wait()
    packed = contract(hot, tok_ref[...], 0, 0).astype(BF)
    for index in range(GROUPS):
        out_refs[index][:, :features] = packed[index * share : (index + 1) * share]
        out_refs[index][:, features:] = packed_meta[index * share : (index + 1) * share]

    copies[3].wait()
    gain = gain_ref[...]
    high = gain.astype(BF).astype(F32)
    middle = (gain - high).astype(BF).astype(F32)
    low = gain - high - middle
    line = lax.broadcasted_iota(jnp.int32, (GAIN_ROWS, width), 0)
    parts = jnp.where(line == 0, high, jnp.where(line == 1, middle, 0.0))
    parts = jnp.where(line == 2, low, parts).astype(BF)
    for ref in part_refs:
        ref[rows:, :width] = parts
        ref[rows:, width:] = jnp.zeros((GAIN_ROWS, width), BF)
    for copy in copies[4:]:
        copy.wait()


def cot_pack_kernel(pieces, share, *refs):
    piece_refs, hot_ref = refs[:pieces], refs[pieces]
    out_refs, full_ref = refs[pieces + 1 : -1], refs[-1]
    me = lax.axis_index("tp")
    rows = hot_ref.shape[0]
    width = piece_refs[0].shape[1] // 2
    features = width * pieces

    def read(ref):
        gain = jnp.sum(ref[rows:, :width].astype(F32), axis=0, keepdims=True)
        return ref[:rows, width:].astype(F32), gain * ref[:rows, :width].astype(F32)

    square_sum = 0.0
    cross_sum = 0.0
    for ref in piece_refs:
        saved, scaled = read(ref)
        square_sum += jnp.sum(saved * saved, axis=1, keepdims=True)
        cross_sum += jnp.sum(saved * scaled, axis=1, keepdims=True)
    inv_rms = lax.rsqrt(square_sum / features + epsilon)
    factor = inv_rms * inv_rms * inv_rms * cross_sum / features
    for index, ref in enumerate(piece_refs):
        saved, scaled = read(ref)
        column = pl.multiple_of(jnp.bitwise_xor(me, index) * width, width)
        full_ref[:, pl.ds(column, width)] = (inv_rms * scaled - saved * factor).astype(BF)
    packed = contract(hot_ref[...], full_ref[...], 0, 0).astype(BF)
    for index in range(GROUPS):
        out_refs[index][...] = packed[index * share : (index + 1) * share]


def route_hots(part_refs, group_size, capacity):
    slots = len(part_refs) * capacity
    hots = []
    for k in range(2):
        blocks = []
        for index, ref in enumerate(part_refs):
            part = ref[...].astype(F32)
            partner = part[:, 2 * k : 2 * k + 1]
            slot = partner * slots + index * capacity + part[:, 2 * k + 1 : 2 * k + 2]
            slot = jnp.where(partner < 0, -1.0, slot).astype(jnp.int32)
            blocks.append(one_hot(slot, group_size * slots))
        hots.append(jnp.concatenate(blocks, axis=0))
    return hots


def token_route_kernel(shifts, group_size, capacity, *refs):
    msg_refs, out_refs = refs[:shifts], refs[shifts : shifts + group_size]
    part_refs, full_ref = refs[shifts + group_size : -1], refs[-1]
    share, width = msg_refs[0].shape
    features = width - META
    slots = shifts * capacity
    _, mine = place(group_size)
    lower = strict_lower(share)
    gates = []
    for index, ref in enumerate(msg_refs):
        row = slice(index * share, (index + 1) * share)
        full_ref[row, :] = ref[:, :features]
        meta = ref[:, features:].astype(F32)
        gates.append((meta[:, 2:3], meta[:, 3:4]))
        experts = [meta[:, k : k + 1].astype(jnp.int32) - 1 for k in range(2)]
        members = [one_hot(e, META) for e in experts]
        before = contract(lower, members[0] + members[1], 1, 0)
        parts = []
        for expert, member in zip(experts, members):
            partner = jnp.where(expert < 0, -1, jnp.bitwise_xor(expert, mine))
            parts.append(partner.astype(F32))
            parts.append(jnp.sum(before * member.astype(F32), axis=1, keepdims=True))
        part_refs[index][...] = lane_of(parts, share).astype(BF)
    hot0, hot1 = route_hots(part_refs, group_size, capacity)
    total = shifts * share
    gate0 = lane_of((jnp.concatenate([g[0] for g in gates], axis=0),), total).astype(BF)
    gate1 = lane_of((jnp.concatenate([g[1] for g in gates], axis=0),), total).astype(BF)
    packed_gate = contract(hot0, gate0, 0, 0) + contract(hot1, gate1, 0, 0)
    packed = contract(hot0 + hot1, full_ref[...], 0, 0)
    for index in range(group_size):
        row = slice(index * slots, (index + 1) * slots)
        out_refs[index][:, :features] = packed[row].astype(BF)
        out_refs[index][:, features:] = packed_gate[row].astype(BF)


def cot_route_kernel(shifts, group_size, capacity, *refs):
    msg_refs, part_refs = refs[:shifts], refs[shifts : 2 * shifts]
    out_refs, full_ref = refs[2 * shifts : -1], refs[-1]
    share = msg_refs[0].shape[0]
    slots = shifts * capacity
    for index, ref in enumerate(msg_refs):
        full_ref[index * share : (index + 1) * share, :] = ref[...]
    hot0, hot1 = route_hots(part_refs, group_size, capacity)
    packed = contract(hot0 + hot1, full_ref[...], 0, 0)
    for index in range(group_size):
        out_refs[index][...] = packed[index * slots : (index + 1) * slots].astype(BF)


def combine_kernel(shifts, group_size, capacity, *refs):
    piece_refs, part_refs = refs[:group_size], refs[group_size : group_size + shifts]
    out_refs = refs[group_size + shifts :]
    share, width = out_refs[0].shape
    features = width - META
    rows = jnp.concatenate([ref[...].astype(F32) for ref in piece_refs], axis=0).astype(BF)
    hot0, hot1 = route_hots(part_refs, group_size, capacity)
    summed = contract(hot0 + hot1, rows[:, :features], 1, 0).astype(BF)
    grad0 = contract(hot0, rows[:, features:], 1, 0)[:, 0:1]
    grad1 = contract(hot1, rows[:, features:], 1, 0)[:, 0:1]
    meta = lane_of((grad0, grad1), shifts * share).astype(BF)
    for index in range(shifts):
        row = slice(index * share, (index + 1) * share)
        out_refs[index][:, :features] = summed[row]
        out_refs[index][:, features:] = meta[row]


def finish_kernel(hot_ref, *refs):
    msg_refs, tok_ref, gates_ref = refs[:GROUPS], refs[-2], refs[-1]
    features = tok_ref.shape[1]
    rows = jnp.concatenate([ref[...] for ref in msg_refs], axis=0)
    hot = hot_ref[...]
    tok_ref[...] = contract(hot, rows[:, :features], 1, 0).astype(BF)
    grads = contract(rows[:, features:].astype(F32).T.astype(BF), hot, 1, 1)
    gates_ref[...] = grads[0:2].astype(BF)


def forward_kernel(*refs):
    count = len(refs) - 6
    piece_refs, (gate_ref, up_ref) = refs[:count], refs[count : count + 2]
    rows_ref, meta_ref, pre_gate_ref, pre_up_ref = refs[count + 2 :]
    slots, features = piece_refs[0].shape[0], rows_ref.shape[1]
    for index, ref in enumerate(piece_refs):
        rows_ref[index * slots : (index + 1) * slots, :] = ref[:, :features]
        meta_ref[index * slots : (index + 1) * slots, :] = ref[:, features:]
    rows = rows_ref[...]
    pre_gate_ref[...] = contract(rows, gate_ref[0], 1, 0)
    pre_up_ref[...] = contract(rows, up_ref[0], 1, 0)


def backward_kernel(group_size, *refs):
    piece_refs = refs[:group_size]
    meta_ref, pre_gate_ref, pre_up_ref, gate_ref, up_ref, down_ref = refs[
        group_size : group_size + 6
    ]
    out_refs = refs[group_size + 6 : 2 * group_size + 6]
    d_gate_ref, d_up_ref, hidden_ref, scaled_ref, cot_ref = refs[2 * group_size + 6 :]
    slots, features = piece_refs[0].shape
    rows = cot_ref.shape[0]
    for index, ref in enumerate(piece_refs):
        cot_ref[index * slots : (index + 1) * slots, :] = ref[...]
    weight = meta_ref[:, 0:1].astype(F32)
    hid_grad = contract(cot_ref[...], down_ref[0], 1, 1)
    pre_gate, pre_up = pre_gate_ref[...], pre_up_ref[...]
    sigmoid_gate = jax.nn.sigmoid(pre_gate)
    activated = pre_gate * sigmoid_gate
    hidden = activated * pre_up
    grad = lane_of((jnp.sum(hidden * hid_grad, axis=1, keepdims=True),), rows).astype(BF)
    d_hidden = weight * hid_grad
    d_gate_ref[...] = (
        d_hidden * pre_up * sigmoid_gate * (1.0 + pre_gate * (1.0 - sigmoid_gate))
    ).astype(BF)
    d_up_ref[...] = (d_hidden * activated).astype(BF)
    hidden_ref[...] = hidden.astype(BF)
    tile = features // FEATURE_TILES
    for start in range(0, features, tile):
        column = slice(start, start + tile)
        back = contract(d_gate_ref[...], gate_ref[0, column, :], 1, 1)
        back = (back + contract(d_up_ref[...], up_ref[0, column, :], 1, 1)).astype(BF)
        for index, ref in enumerate(out_refs):
            ref[:, column] = back[index * slots : (index + 1) * slots]
    for index, ref in enumerate(out_refs):
        ref[:, features:] = grad[index * slots : (index + 1) * slots]
    scaled_ref[...] = (weight * cot_ref[...].astype(F32)).astype(BF)


def weight_kernel(sets, *refs):
    rows, d_gate, d_up, hidden, scaled = (refs[k * sets : (k + 1) * sets] for k in range(5))
    grad_gate_ref, grad_up_ref, grad_down_ref, both_ref, turned_ref = refs[5 * sets :]
    hidden_width = hidden[0].shape[1]

    @pl.when(pl.program_id(0) == 0)
    def _():
        first = 0
        for gate, up, hid in zip(d_gate, d_up, hidden):
            last = first + gate.shape[0]
            both_ref[first:last, :hidden_width] = gate[...]
            both_ref[first:last, hidden_width:] = up[...]
            turned_ref[:, first:last] = hid[...].T
            first = last

    tokens = jnp.concatenate([ref[...] for ref in rows], axis=0)
    both = contract(tokens, both_ref[...], 0, 0)
    grad_gate_ref[0] = both[:, :hidden_width].astype(BF)
    grad_up_ref[0] = both[:, hidden_width:].astype(BF)
    cots = jnp.concatenate([ref[...] for ref in scaled], axis=0)
    grad_down_ref[0] = contract(turned_ref[...], cots, 1, 0).astype(BF)


def forward_call(pieces, w_gate, w_up):
    features, hidden = w_gate.shape[1:]
    rows = sum(p.shape[0] for p in pieces)
    return call(
        forward_kernel,
        [(rows, features), (rows, META), (rows, hidden, F32), (rows, hidden, F32)],
        [*pieces, w_gate, w_up],
        flops=4 * rows * features * hidden,
        limit=BIG_VMEM,
    )


def backward_call(pieces, *held):
    features, hidden = held[3].shape[1:]
    slots = pieces[0].shape[0]
    rows = slots * len(pieces)
    result = call(
        functools.partial(backward_kernel, len(pieces)),
        [(slots, features + META)] * len(pieces) + [(rows, hidden)] * 3 + [(rows, features)],
        [*pieces, *held],
        scratch=[((rows, features), BF)],
        flops=6 * rows * features * hidden,
        limit=BIG_VMEM,
    )
    return result[: len(pieces)], result[len(pieces) :]


def weight_call(rows, kept):
    d_gate, d_up, hidden, scaled = ([k[i] for k in kept] for i in range(4))
    total, features = sum(r.shape[0] for r in rows), rows[0].shape[1]
    width = hidden[0].shape[1]
    tile = features // FEATURE_TILES
    whole = lambda a: pl.BlockSpec(a.shape, lambda d: (0, 0))
    return pl.pallas_call(
        functools.partial(weight_kernel, len(kept)),
        grid=(FEATURE_TILES,),
        out_shape=[
            jax.ShapeDtypeStruct((1, features, width), BF),
            jax.ShapeDtypeStruct((1, features, width), BF),
            jax.ShapeDtypeStruct((1, width, features), BF),
        ],
        in_specs=[pl.BlockSpec((a.shape[0], tile), lambda d: (0, d)) for a in rows]
        + [whole(a) for a in (*d_gate, *d_up, *hidden)]
        + [pl.BlockSpec((a.shape[0], tile), lambda d: (0, d)) for a in scaled],
        out_specs=[
            pl.BlockSpec((1, tile, width), lambda d: (0, d, 0)),
            pl.BlockSpec((1, tile, width), lambda d: (0, d, 0)),
            pl.BlockSpec((1, width, tile), lambda d: (0, 0, d)),
        ],
        scratch_shapes=[pltpu.VMEM((total, 2 * width), BF), pltpu.VMEM((width, total), BF)],
        compiler_params=pltpu.CompilerParams(vmem_limit_bytes=BIG_VMEM),
        cost_estimate=pl.CostEstimate(
            flops=6 * total * features * width,
            bytes_accessed=6 * features * width + 4 * total * features + 6 * total * width,
            transcendentals=0,
        ),
    )(*rows, *d_gate, *d_up, *hidden, *scaled)


def call(kernel, outs, args, scratch=(), copies=0, flops=0, limit=SMALL_VMEM):
    outs = [jax.ShapeDtypeStruct(o[:2], o[2] if len(o) > 2 else BF) for o in outs]
    size = sum(a.size * a.dtype.itemsize for a in (*args, *outs))
    return pl.pallas_call(
        kernel,
        out_shape=outs,
        in_specs=[pl.BlockSpec(memory_space=pltpu.HBM if copies else pltpu.VMEM)] * len(args),
        out_specs=[pl.BlockSpec(memory_space=pltpu.VMEM)] * len(outs),
        scratch_shapes=[pltpu.VMEM(shape, dtype) for shape, dtype in scratch]
        + [pltpu.SemaphoreType.DMA((copies,))] * bool(copies),
        compiler_params=pltpu.CompilerParams(vmem_limit_bytes=limit),
        cost_estimate=pl.CostEstimate(flops=flops, bytes_accessed=size, transcendentals=0),
    )(*args)


def local(tokens, routes, gates, w_gate, w_up, w_down, moe_out, norm_gain, out_grad):
    devices = lax.axis_size(AXES)
    pieces = lax.axis_size("tp")
    group_size = devices // GROUPS
    tok_rows, features = tokens.shape
    capacity = 4 * tok_rows // devices
    share = 3 * tok_rows // 8
    wide = features + META

    def over_tp(array, bits):
        pairs = [(d, d ^ bits) for d in range(pieces)]
        return lax.ppermute(array, "tp", pairs)

    def over_plane(array, bits):
        pairs = [
            (d, d // group_size * group_size + (d % group_size ^ bits)) for d in range(devices)
        ]
        return lax.ppermute(array, AXES, pairs)

    def over_z(array, shift):
        pairs = [(d, (d + shift * group_size) % devices) for d in range(devices)]
        return lax.ppermute(array, AXES, pairs)

    part = [(tok_rows + GAIN_ROWS, 2 * moe_out.shape[1])] * pieces
    *out, hot = call(
        functools.partial(head_kernel, pieces, group_size, share),
        part + [(share, wide)] * GROUPS + [(tok_rows, GROUPS * share)],
        (tokens, routes.T, gates.T, moe_out, norm_gain[None, :], out_grad),
        scratch=[
            ((tok_rows, features), BF),
            (routes.shape[::-1], jnp.int32),
            (gates.shape[::-1], F32),
            ((1, norm_gain.shape[0]), F32),
            ((8, tok_rows), F32),
        ],
        copies=4 + 2 * pieces,
        limit=HEAD_VMEM,
        flops=2 * tok_rows * GROUPS * share * wide,
    )
    split, tok_msgs = out[:pieces], out[pieces:]
    split = [split[0]] + [over_tp(split[m], m) for m in range(1, pieces)]
    tok_at = {0: tok_msgs[0]}
    for s in TOKEN_SHIFTS:
        tok_at[s] = over_z(tok_msgs[s], s)
    cot_msgs = call(
        functools.partial(cot_pack_kernel, pieces, share),
        [(share, features)] * GROUPS,
        (*split, hot),
        scratch=[((tok_rows, features), BF)],
        flops=2 * tok_rows * GROUPS * share * features,
    )
    cot_at = {0: cot_msgs[0]}
    for s in COT_SHIFTS:
        cot_at[s] = over_z(cot_msgs[s], s)

    parts, tok_in, cot_in = {}, [], []
    for group in TOKEN_SETS:
        count = len(group)
        slots = count * capacity
        out = call(
            functools.partial(token_route_kernel, count, group_size, capacity),
            [(slots, wide)] * group_size + [(share, META)] * count,
            [tok_at[s] for s in group],
            scratch=[((count * share, features), BF)],
            flops=2 * count * share * group_size * slots * wide,
        )
        parts.update(zip(group, out[group_size:]))
        tok_in.append([out[0]] + [over_plane(out[m], m) for m in range(1, group_size)])
    for group in SETS:
        count = len(group)
        slots = count * capacity
        out = call(
            functools.partial(cot_route_kernel, count, group_size, capacity),
            [(slots, features)] * group_size,
            [cot_at[s] for s in group] + [parts[s] for s in group],
            scratch=[((count * share, features), BF)],
            flops=2 * count * share * group_size * slots * features,
        )
        cot_in.append([out[0]] + [over_plane(out[m], m) for m in range(1, group_size)])

    backs, kept, row_blocks = [], [], []
    for group, cots in zip(SETS, cot_in):
        rows, *held = forward_call(tok_in[TOKEN_SETS.index(group)], w_gate, w_up)
        back, keep = backward_call(cots, *held, w_gate, w_up, w_down)
        backs.append([back[0]] + [over_plane(back[m], m) for m in range(1, group_size)])
        kept.append(keep)
        row_blocks.append(rows)
    grad_gate, grad_up, grad_down = weight_call(row_blocks, kept)

    home = {}
    for group, back in zip(SETS, backs):
        count = len(group)
        out = call(
            functools.partial(combine_kernel, count, group_size, capacity),
            [(share, wide)] * count,
            [*back] + [parts[s] for s in group],
            flops=2 * count * share * group_size * count * capacity * wide,
        )
        for s, array in zip(group, out):
            home[s] = over_z(array, -s) if s else array
    token_grad, gates_grad = call(
        finish_kernel,
        [(tok_rows, features), (routes.shape[1], tok_rows)],
        [hot] + [home[s] for s in range(GROUPS)],
        flops=2 * hot.size * wide,
    )
    return (token_grad, gates_grad.T, grad_gate, grad_up, grad_down)


def solution(mesh):
    in_specs = (
        P(AXES, None),
        P(AXES, None),
        P(AXES, None),
        P(AXES, None, None),
        P(AXES, None, None),
        P(AXES, None, None),
        P("ep", "tp"),
        P("tp"),
        P("ep", "tp"),
    )
    out_specs = (
        P(AXES, None),
        P(AXES, None),
        P(AXES, None, None),
        P(AXES, None, None),
        P(AXES, None, None),
    )

    return jax.shard_map(local, mesh=mesh, in_specs=in_specs, out_specs=out_specs, check_vma=False)
```

```python
import functools

import jax
import jax.numpy as jnp
from jax import lax
from jax.experimental import pallas as pl
from jax.experimental.pallas import tpu as pltpu
from jax.sharding import PartitionSpec as P


epsilon = 1e-06
AXES = ("ep", "tp")
GROUPS = 4
META = 128
LANES = 128
LINES = 8
GAIN_ROWS = 16
FEATURE_TILES = 4
SMALL_VMEM = 16 * 2**20
BIG_VMEM = 24 * 2**20
HEAD_VMEM = 60 * 2**20
TOKEN_SETS = ((3, 0), (1, 2))
SETS = ((1, 2), (3, 0))
TOKEN_SHIFTS = (3, 1, 2)
COT_SHIFTS = (1, 2, 3)
BF = jnp.bfloat16
F32 = jnp.float32


def contract(left, right, left_dim, right_dim):
    return lax.dot_general(
        left, right, (((left_dim,), (right_dim,)), ((), ())), preferred_element_type=F32
    )


def one_hot(column, width):
    lanes = lax.broadcasted_iota(jnp.int32, (column.shape[0], width), 1)
    return jnp.where(column == lanes, 1.0, 0.0).astype(BF)


def strict_lower(rows):
    above = lax.broadcasted_iota(jnp.int32, (rows, rows), 1)
    below = lax.broadcasted_iota(jnp.int32, (rows, rows), 0)
    return jnp.where(above < below, 1.0, 0.0).astype(BF)


def lane_of(column_values, rows):
    lanes = lax.broadcasted_iota(jnp.int32, (rows, META), 1)
    result = jnp.zeros((rows, META), F32)
    for lane, column in enumerate(column_values):
        result = jnp.where(lanes == lane, column, result)
    return result


def plane_shape(slots, features):
    return (slots * (features // LANES) + LINES, LANES)


def put_columns(ref, values, first, slots):
    for tile in range(values.shape[1] // LANES):
        row = (first // LANES + tile) * slots
        ref[row : row + slots, :] = values[:, tile * LANES : (tile + 1) * LANES]


def get_columns(target_ref, first, ref, slots):
    for tile in range((ref.shape[0] - LINES) // slots):
        block = ref[tile * slots : (tile + 1) * slots, :]
        target_ref[first : first + slots, tile * LANES : (tile + 1) * LANES] = block


def put_line(ref, lines, index, slots):
    first = index * slots // LANES * LANES
    ref[ref.shape[0] - LINES :, :] = lines[:LINES, first : first + LANES].astype(BF)


def get_line(ref):
    return ref[ref.shape[0] - LINES :, :].astype(F32)[0:1, :]


def place(group_size):
    flat = lax.axis_index("ep") * lax.axis_size("tp") + lax.axis_index("tp")
    return lax.div(flat, group_size), lax.rem(flat, group_size)


def head_kernel(pieces, group_size, share, *refs):
    tok_hbm, routes_hbm, gates_hbm, moe_hbm, gain_hbm, grad_hbm = refs[:6]
    part_refs, refs = refs[6 : 6 + pieces], refs[6 + pieces :]
    out_refs, hot_ref = refs[:GROUPS], refs[GROUPS]
    tok_ref, routes_ref, gates_ref, gain_ref, lines_ref, sems = refs[GROUPS + 1 :]
    rows, _ = tok_ref.shape
    width = moe_hbm.shape[1]
    me = lax.axis_index("tp")
    plane, _ = place(group_size)

    sources = [
        (routes_hbm, routes_ref),
        (gates_hbm, gates_ref),
        (tok_hbm, tok_ref),
        (gain_hbm, gain_ref),
    ]
    for index, ref in enumerate(part_refs):
        block = pl.ds(pl.multiple_of(jnp.bitwise_xor(me, index) * rows, rows), rows)
        sources.append((grad_hbm.at[block, :], ref.at[pl.ds(0, rows), pl.ds(0, width)]))
        sources.append((moe_hbm.at[block, :], ref.at[pl.ds(0, rows), pl.ds(width, width)]))
    copies = [pltpu.make_async_copy(a, b, sems.at[i]) for i, (a, b) in enumerate(sources)]
    for copy in copies:
        copy.start()

    lines_ref[...] = jnp.zeros_like(lines_ref)
    copies[0].wait()
    copies[1].wait()
    lines_ref[0:2, :] = routes_ref[...].astype(F32)
    lines_ref[2:4, :] = gates_ref[...]
    unit_row = lax.broadcasted_iota(jnp.int32, (rows, rows), 0)
    unit_col = lax.broadcasted_iota(jnp.int32, (rows, rows), 1)
    unit = jnp.where(unit_row == unit_col, 1.0, 0.0).astype(BF)
    columns = contract(unit, lines_ref[...].astype(BF), 1, 1)
    first = columns[:, 0:1].astype(jnp.int32)
    second = columns[:, 1:2].astype(jnp.int32)
    group = lax.div(first, group_size)
    shift = lax.rem(group - plane + GROUPS, GROUPS)
    member = one_hot(shift, META)
    before = contract(strict_lower(rows), member, 1, 0)
    rank = jnp.sum(before * member.astype(F32), axis=1, keepdims=True).astype(jnp.int32)
    hot = one_hot(shift * share + rank, GROUPS * share)
    hot_ref[...] = hot
    base = group * group_size
    meta = lane_of(
        (
            (first - base + 1).astype(F32),
            (second - base + 1).astype(F32),
            columns[:, 2:3],
            columns[:, 3:4],
        ),
        rows,
    ).astype(BF)
    lines = []
    for index in range(GROUPS):
        slot = jnp.where(shift == index, rank, -1)
        lines.append(contract(meta, one_hot(slot, LANES), 0, 0))
    copies[2].wait()
    packed = contract(hot, tok_ref[...], 0, 0).astype(BF)
    for index, ref in enumerate(out_refs):
        put_columns(ref, packed[index * share : (index + 1) * share], 0, share)
        put_line(ref, lines[index], 0, share)

    copies[3].wait()
    gain = gain_ref[...]
    high = gain.astype(BF).astype(F32)
    middle = (gain - high).astype(BF).astype(F32)
    low = gain - high - middle
    line = lax.broadcasted_iota(jnp.int32, (GAIN_ROWS, width), 0)
    parts = jnp.where(line == 0, high, jnp.where(line == 1, middle, 0.0))
    parts = jnp.where(line == 2, low, parts).astype(BF)
    for ref in part_refs:
        ref[rows:, :width] = parts
        ref[rows:, width:] = jnp.zeros((GAIN_ROWS, width), BF)
    for copy in copies[4:]:
        copy.wait()


def cot_pack_kernel(pieces, share, *refs):
    piece_refs, hot_ref = refs[:pieces], refs[pieces]
    out_refs, full_ref = refs[pieces + 1 : -1], refs[-1]
    me = lax.axis_index("tp")
    rows = hot_ref.shape[0]
    width = piece_refs[0].shape[1] // 2
    features = width * pieces

    def read(ref):
        gain = jnp.sum(ref[rows:, :width].astype(F32), axis=0, keepdims=True)
        return ref[:rows, width:].astype(F32), gain * ref[:rows, :width].astype(F32)

    square_sum = 0.0
    cross_sum = 0.0
    for ref in piece_refs:
        saved, scaled = read(ref)
        square_sum += jnp.sum(saved * saved, axis=1, keepdims=True)
        cross_sum += jnp.sum(saved * scaled, axis=1, keepdims=True)
    inv_rms = lax.rsqrt(square_sum / features + epsilon)
    factor = inv_rms * inv_rms * inv_rms * cross_sum / features
    for index, ref in enumerate(piece_refs):
        saved, scaled = read(ref)
        column = pl.multiple_of(jnp.bitwise_xor(me, index) * width, width)
        full_ref[:, pl.ds(column, width)] = (inv_rms * scaled - saved * factor).astype(BF)
    packed = contract(hot_ref[...], full_ref[...], 0, 0).astype(BF)
    for index in range(GROUPS):
        out_refs[index][...] = packed[index * share : (index + 1) * share]


def route_hots(part_refs, group_size, capacity):
    slots = len(part_refs) * capacity
    hots = []
    for k in range(2):
        blocks = []
        for index, ref in enumerate(part_refs):
            part = ref[...].astype(F32)
            partner = part[:, 2 * k : 2 * k + 1]
            slot = partner * slots + index * capacity + part[:, 2 * k + 1 : 2 * k + 2]
            slot = jnp.where(partner < 0, -1.0, slot).astype(jnp.int32)
            blocks.append(one_hot(slot, group_size * slots))
        hots.append(jnp.concatenate(blocks, axis=0))
    return hots


def token_route_kernel(shifts, group_size, capacity, *refs):
    msg_refs, out_refs = refs[:shifts], refs[shifts : shifts + group_size]
    part_refs, full_ref = refs[shifts + group_size : -1], refs[-1]
    share = part_refs[0].shape[0]
    slots = shifts * capacity
    _, mine = place(group_size)
    lower = strict_lower(share)
    gates = []
    for index, ref in enumerate(msg_refs):
        get_columns(full_ref, index * share, ref, share)
        meta = ref[ref.shape[0] - LINES :, :].astype(F32).T[:share, :]
        gates.append((meta[:, 2:3], meta[:, 3:4]))
        experts = [meta[:, k : k + 1].astype(jnp.int32) - 1 for k in range(2)]
        members = [one_hot(e, META) for e in experts]
        before = contract(lower, members[0] + members[1], 1, 0)
        parts = []
        for expert, member in zip(experts, members):
            partner = jnp.where(expert < 0, -1, jnp.bitwise_xor(expert, mine))
            parts.append(partner.astype(F32))
            parts.append(jnp.sum(before * member.astype(F32), axis=1, keepdims=True))
        part_refs[index][...] = lane_of(parts, share).astype(BF)
    hot0, hot1 = route_hots(part_refs, group_size, capacity)
    total = shifts * share
    gate0 = lane_of((jnp.concatenate([g[0] for g in gates], axis=0),), total).astype(BF)
    gate1 = lane_of((jnp.concatenate([g[1] for g in gates], axis=0),), total).astype(BF)
    lines = contract(gate0, hot0, 0, 0) + contract(gate1, hot1, 0, 0)
    packed = contract(hot0 + hot1, full_ref[...], 0, 0)
    for index, ref in enumerate(out_refs):
        put_columns(ref, packed[index * slots : (index + 1) * slots].astype(BF), 0, slots)
        put_line(ref, lines, index, slots)


def cot_route_kernel(shifts, group_size, capacity, *refs):
    msg_refs, part_refs = refs[:shifts], refs[shifts : 2 * shifts]
    out_refs, full_ref = refs[2 * shifts : -1], refs[-1]
    share = msg_refs[0].shape[0]
    slots = shifts * capacity
    for index, ref in enumerate(msg_refs):
        full_ref[index * share : (index + 1) * share, :] = ref[...]
    hot0, hot1 = route_hots(part_refs, group_size, capacity)
    packed = contract(hot0 + hot1, full_ref[...], 0, 0)
    for index in range(group_size):
        out_refs[index][...] = packed[index * slots : (index + 1) * slots].astype(BF)


def combine_kernel(shifts, group_size, capacity, *refs):
    piece_refs, part_refs = refs[:group_size], refs[group_size : group_size + shifts]
    out_refs, rows_ref = refs[group_size + shifts : -1], refs[-1]
    share = part_refs[0].shape[0]
    slots = shifts * capacity
    lanes = lax.broadcasted_iota(jnp.int32, (1, LANES), 1)
    lines = [jnp.zeros((1, LANES), F32) for _ in range(group_size * slots // LANES)]
    for index, ref in enumerate(piece_refs):
        get_columns(rows_ref, index * slots, ref, slots)
        tile, first = divmod(index * slots, LANES)
        mine = (lanes >= first) & (lanes < first + slots)
        lines[tile] = jnp.where(mine, get_line(ref), lines[tile])
    line = jnp.concatenate(lines, axis=1)
    hot0, hot1 = route_hots(part_refs, group_size, capacity)
    summed = contract(hot0 + hot1, rows_ref[...], 1, 0).astype(BF)
    grad0 = jnp.sum(hot0.astype(F32) * line, axis=1, keepdims=True)
    grad1 = jnp.sum(hot1.astype(F32) * line, axis=1, keepdims=True)
    meta = lane_of((grad0, grad1), shifts * share)
    empty = jnp.zeros((LANES - share, META), F32)
    for index, ref in enumerate(out_refs):
        row = slice(index * share, (index + 1) * share)
        put_columns(ref, summed[row], 0, share)
        put_line(ref, jnp.concatenate([meta[row], empty], axis=0).T, 0, share)


def finish_kernel(hot_ref, *refs):
    msg_refs, tok_ref, gates_ref, rows_ref = refs[:GROUPS], *refs[-3:]
    share = rows_ref.shape[0] // GROUPS
    hot = hot_ref[...]
    grads = 0.0
    for index, ref in enumerate(msg_refs):
        get_columns(rows_ref, index * share, ref, share)
        lines = ref[ref.shape[0] - LINES :, :share]
        grads += contract(lines, hot[:, index * share : (index + 1) * share], 1, 1)
    tok_ref[...] = contract(hot, rows_ref[...], 1, 0).astype(BF)
    gates_ref[...] = grads[0:2].astype(BF)


def forward_kernel(*refs):
    count = len(refs) - 6
    piece_refs, (gate_ref, up_ref) = refs[:count], refs[count : count + 2]
    rows_ref, meta_ref, pre_gate_ref, pre_up_ref = refs[count + 2 :]
    slots = rows_ref.shape[0] // count
    line = lax.broadcasted_iota(jnp.int32, (slots, LANES), 0)
    lane = lax.broadcasted_iota(jnp.int32, (slots, LANES), 1)
    for index, ref in enumerate(piece_refs):
        get_columns(rows_ref, index * slots, ref, slots)
        own = lane == line + index * slots % LANES
        gate = jnp.sum(jnp.where(own, get_line(ref), 0.0), axis=1, keepdims=True)
        gate = jnp.broadcast_to(gate, (slots, META)).astype(BF)
        meta_ref[index * slots : (index + 1) * slots, :] = gate
    rows = rows_ref[...]
    pre_gate_ref[...] = contract(rows, gate_ref[0], 1, 0)
    pre_up_ref[...] = contract(rows, up_ref[0], 1, 0)


def backward_kernel(group_size, *refs):
    piece_refs = refs[:group_size]
    meta_ref, pre_gate_ref, pre_up_ref, gate_ref, up_ref, down_ref = refs[
        group_size : group_size + 6
    ]
    out_refs = refs[group_size + 6 : 2 * group_size + 6]
    d_gate_ref, d_up_ref, hidden_ref, scaled_ref, cot_ref = refs[2 * group_size + 6 :]
    slots, features = piece_refs[0].shape
    rows = cot_ref.shape[0]
    for index, ref in enumerate(piece_refs):
        cot_ref[index * slots : (index + 1) * slots, :] = ref[...]
    weight = meta_ref[:, 0:1].astype(F32)
    hid_grad = contract(cot_ref[...], down_ref[0], 1, 1)
    pre_gate, pre_up = pre_gate_ref[...], pre_up_ref[...]
    sigmoid_gate = jax.nn.sigmoid(pre_gate)
    activated = pre_gate * sigmoid_gate
    hidden = activated * pre_up
    lines = lane_of((jnp.sum(hidden * hid_grad, axis=1, keepdims=True),), rows).T
    d_hidden = weight * hid_grad
    d_gate_ref[...] = (
        d_hidden * pre_up * sigmoid_gate * (1.0 + pre_gate * (1.0 - sigmoid_gate))
    ).astype(BF)
    d_up_ref[...] = (d_hidden * activated).astype(BF)
    hidden_ref[...] = hidden.astype(BF)
    tile = features // FEATURE_TILES
    for start in range(0, features, tile):
        column = slice(start, start + tile)
        back = contract(d_gate_ref[...], gate_ref[0, column, :], 1, 1)
        back = (back + contract(d_up_ref[...], up_ref[0, column, :], 1, 1)).astype(BF)
        for index, ref in enumerate(out_refs):
            put_columns(ref, back[index * slots : (index + 1) * slots], start, slots)
    for index, ref in enumerate(out_refs):
        put_line(ref, lines, index, slots)
    scaled_ref[...] = (weight * cot_ref[...].astype(F32)).astype(BF)


def weight_kernel(sets, *refs):
    rows, d_gate, d_up, hidden, scaled = (refs[k * sets : (k + 1) * sets] for k in range(5))
    grad_gate_ref, grad_up_ref, grad_down_ref, both_ref, turned_ref = refs[5 * sets :]
    hidden_width = hidden[0].shape[1]

    @pl.when(pl.program_id(0) == 0)
    def _():
        first = 0
        for gate, up, hid in zip(d_gate, d_up, hidden):
            last = first + gate.shape[0]
            both_ref[first:last, :hidden_width] = gate[...]
            both_ref[first:last, hidden_width:] = up[...]
            turned_ref[:, first:last] = hid[...].T
            first = last

    tokens = jnp.concatenate([ref[...] for ref in rows], axis=0)
    both = contract(tokens, both_ref[...], 0, 0)
    grad_gate_ref[0] = both[:, :hidden_width].astype(BF)
    grad_up_ref[0] = both[:, hidden_width:].astype(BF)
    cots = jnp.concatenate([ref[...] for ref in scaled], axis=0)
    grad_down_ref[0] = contract(turned_ref[...], cots, 1, 0).astype(BF)


def forward_call(pieces, w_gate, w_up):
    features, hidden = w_gate.shape[1:]
    rows = sum((p.shape[0] - LINES) * LANES // features for p in pieces)
    return call(
        forward_kernel,
        [(rows, features), (rows, META), (rows, hidden, F32), (rows, hidden, F32)],
        [*pieces, w_gate, w_up],
        flops=4 * rows * features * hidden,
        limit=BIG_VMEM,
    )


def backward_call(pieces, *held):
    features, hidden = held[3].shape[1:]
    slots = pieces[0].shape[0]
    rows = slots * len(pieces)
    result = call(
        functools.partial(backward_kernel, len(pieces)),
        [plane_shape(slots, features)] * len(pieces) + [(rows, hidden)] * 3 + [(rows, features)],
        [*pieces, *held],
        scratch=[((rows, features), BF)],
        flops=6 * rows * features * hidden,
        limit=BIG_VMEM,
    )
    return result[: len(pieces)], result[len(pieces) :]


def weight_call(rows, kept):
    d_gate, d_up, hidden, scaled = ([k[i] for k in kept] for i in range(4))
    total, features = sum(r.shape[0] for r in rows), rows[0].shape[1]
    width = hidden[0].shape[1]
    tile = features // FEATURE_TILES
    whole = lambda a: pl.BlockSpec(a.shape, lambda d: (0, 0))
    return pl.pallas_call(
        functools.partial(weight_kernel, len(kept)),
        grid=(FEATURE_TILES,),
        out_shape=[
            jax.ShapeDtypeStruct((1, features, width), BF),
            jax.ShapeDtypeStruct((1, features, width), BF),
            jax.ShapeDtypeStruct((1, width, features), BF),
        ],
        in_specs=[pl.BlockSpec((a.shape[0], tile), lambda d: (0, d)) for a in rows]
        + [whole(a) for a in (*d_gate, *d_up, *hidden)]
        + [pl.BlockSpec((a.shape[0], tile), lambda d: (0, d)) for a in scaled],
        out_specs=[
            pl.BlockSpec((1, tile, width), lambda d: (0, d, 0)),
            pl.BlockSpec((1, tile, width), lambda d: (0, d, 0)),
            pl.BlockSpec((1, width, tile), lambda d: (0, 0, d)),
        ],
        scratch_shapes=[pltpu.VMEM((total, 2 * width), BF), pltpu.VMEM((width, total), BF)],
        compiler_params=pltpu.CompilerParams(vmem_limit_bytes=BIG_VMEM),
        cost_estimate=pl.CostEstimate(
            flops=6 * total * features * width,
            bytes_accessed=6 * features * width + 4 * total * features + 6 * total * width,
            transcendentals=0,
        ),
    )(*rows, *d_gate, *d_up, *hidden, *scaled)


def call(kernel, outs, args, scratch=(), copies=0, flops=0, limit=SMALL_VMEM):
    outs = [jax.ShapeDtypeStruct(o[:2], o[2] if len(o) > 2 else BF) for o in outs]
    size = sum(a.size * a.dtype.itemsize for a in (*args, *outs))
    return pl.pallas_call(
        kernel,
        out_shape=outs,
        in_specs=[pl.BlockSpec(memory_space=pltpu.HBM if copies else pltpu.VMEM)] * len(args),
        out_specs=[pl.BlockSpec(memory_space=pltpu.VMEM)] * len(outs),
        scratch_shapes=[pltpu.VMEM(shape, dtype) for shape, dtype in scratch]
        + [pltpu.SemaphoreType.DMA((copies,))] * bool(copies),
        compiler_params=pltpu.CompilerParams(vmem_limit_bytes=limit),
        cost_estimate=pl.CostEstimate(flops=flops, bytes_accessed=size, transcendentals=0),
    )(*args)


def local(tokens, routes, gates, w_gate, w_up, w_down, moe_out, norm_gain, out_grad):
    devices = lax.axis_size(AXES)
    pieces = lax.axis_size("tp")
    group_size = devices // GROUPS
    tok_rows, features = tokens.shape
    capacity = 4 * tok_rows // devices
    share = 3 * tok_rows // 8
    wide = features + META

    def over_tp(array, bits):
        pairs = [(d, d ^ bits) for d in range(pieces)]
        return lax.ppermute(array, "tp", pairs)

    def over_plane(array, bits):
        pairs = [
            (d, d // group_size * group_size + (d % group_size ^ bits)) for d in range(devices)
        ]
        return lax.ppermute(array, AXES, pairs)

    def over_z(array, shift):
        pairs = [(d, (d + shift * group_size) % devices) for d in range(devices)]
        return lax.ppermute(array, AXES, pairs)

    part = [(tok_rows + GAIN_ROWS, 2 * moe_out.shape[1])] * pieces
    *out, hot = call(
        functools.partial(head_kernel, pieces, group_size, share),
        part + [plane_shape(share, features)] * GROUPS + [(tok_rows, GROUPS * share)],
        (tokens, routes.T, gates.T, moe_out, norm_gain[None, :], out_grad),
        scratch=[
            ((tok_rows, features), BF),
            (routes.shape[::-1], jnp.int32),
            (gates.shape[::-1], F32),
            ((1, norm_gain.shape[0]), F32),
            ((8, tok_rows), F32),
        ],
        copies=4 + 2 * pieces,
        limit=HEAD_VMEM,
        flops=2 * tok_rows * GROUPS * share * wide,
    )
    split, tok_msgs = out[:pieces], out[pieces:]
    split = [split[0]] + [over_tp(split[m], m) for m in range(1, pieces)]
    tok_at = {0: tok_msgs[0]}
    for s in TOKEN_SHIFTS:
        tok_at[s] = over_z(tok_msgs[s], s)
    cot_msgs = call(
        functools.partial(cot_pack_kernel, pieces, share),
        [(share, features)] * GROUPS,
        (*split, hot),
        scratch=[((tok_rows, features), BF)],
        flops=2 * tok_rows * GROUPS * share * features,
    )
    cot_at = {0: cot_msgs[0]}
    for s in COT_SHIFTS:
        cot_at[s] = over_z(cot_msgs[s], s)

    parts, tok_in, cot_in = {}, [], []
    for group in TOKEN_SETS:
        count = len(group)
        slots = count * capacity
        out = call(
            functools.partial(token_route_kernel, count, group_size, capacity),
            [plane_shape(slots, features)] * group_size + [(share, META)] * count,
            [tok_at[s] for s in group],
            scratch=[((count * share, features), BF)],
            flops=2 * count * share * group_size * slots * wide,
        )
        parts.update(zip(group, out[group_size:]))
        tok_in.append([out[0]] + [over_plane(out[m], m) for m in range(1, group_size)])
    for group in SETS:
        count = len(group)
        slots = count * capacity
        out = call(
            functools.partial(cot_route_kernel, count, group_size, capacity),
            [(slots, features)] * group_size,
            [cot_at[s] for s in group] + [parts[s] for s in group],
            scratch=[((count * share, features), BF)],
            flops=2 * count * share * group_size * slots * features,
        )
        cot_in.append([out[0]] + [over_plane(out[m], m) for m in range(1, group_size)])

    backs, kept, row_blocks = [], [], []
    for group, cots in zip(SETS, cot_in):
        rows, *held = forward_call(tok_in[TOKEN_SETS.index(group)], w_gate, w_up)
        back, keep = backward_call(cots, *held, w_gate, w_up, w_down)
        backs.append([back[0]] + [over_plane(back[m], m) for m in range(1, group_size)])
        kept.append(keep)
        row_blocks.append(rows)
    grad_gate, grad_up, grad_down = weight_call(row_blocks, kept)

    home = {}
    for group, back in zip(SETS, backs):
        count = len(group)
        out = call(
            functools.partial(combine_kernel, count, group_size, capacity),
            [plane_shape(share, features)] * count,
            [*back] + [parts[s] for s in group],
            scratch=[((group_size * count * capacity, features), BF)],
            flops=2 * count * share * group_size * count * capacity * wide,
        )
        for s, array in zip(group, out):
            home[s] = over_z(array, -s) if s else array
    token_grad, gates_grad = call(
        finish_kernel,
        [(tok_rows, features), (routes.shape[1], tok_rows)],
        [hot] + [home[s] for s in range(GROUPS)],
        scratch=[((GROUPS * share, features), BF)],
        flops=2 * hot.size * wide,
    )
    return (token_grad, gates_grad.T, grad_gate, grad_up, grad_down)


def solution(mesh):
    in_specs = (
        P(AXES, None),
        P(AXES, None),
        P(AXES, None),
        P(AXES, None, None),
        P(AXES, None, None),
        P(AXES, None, None),
        P("ep", "tp"),
        P("tp"),
        P("ep", "tp"),
    )
    out_specs = (
        P(AXES, None),
        P(AXES, None),
        P(AXES, None, None),
        P(AXES, None, None),
        P(AXES, None, None),
    )

    return jax.shard_map(local, mesh=mesh, in_specs=in_specs, out_specs=out_specs, check_vma=False)
```
